256 devices in a mesh: ep: 16 (over y, x), tp: 16 (over z, core).
Axes of the slice: x: 4, y: 4, z: 8, core: 2. Of those that a mesh axis runs over, the one named last changes fastest.
Arguments:
- tokens: bfloat16 [1024, 2048], P(('ep', 'tp')), may hold values from -6 to 6
- lengths: int32 [1024], P(('ep', 'tp')), may hold values from 64 to 1024
- cache_latent: bfloat16 [1024, 1024, 512], P(('ep', 'tp')), may hold values from -6 to 6
- cache_rope_key: bfloat16 [1024, 1024, 32], P(('ep', 'tp')), may hold values from -1000 to 1000
- route_ids: int32 [1024, 4], P('ep'), may hold values from 0 to 255, all different within a row; in each aligned block of 64 rows (0 to 63, 64 to 127, ...) at most 2 rows name the same one
- route_weights: float32 [1024, 4], P('ep'), may hold values from 0.2 to 2
- attn_gain: float32 [2048], replicated, may hold values from 0.1 to 1.9
- w_query_nope: bfloat16 [2048, 16, 64], P(None, 'tp'), may hold values from -0.125 to 0.125
- w_query_rope: bfloat16 [2048, 16, 32], P(None, 'tp'), may hold values from -0.125 to 0.125
- w_latent_down: bfloat16 [2048, 512], P(None, 'tp'), may hold values from -0.125 to 0.125
- w_key_rope: bfloat16 [2048, 32], replicated, may hold values from -0.125 to 0.125
- latent_gain: float32 [512], replicated, may hold values from 0.1 to 1.9
- w_key_up: bfloat16 [512, 16, 64], P(None, 'tp'), may hold values from -0.75 to 0.75
- w_value_up: bfloat16 [512, 16, 64], P(None, 'tp'), may hold values from -0.25 to 0.25
- w_attn_out: bfloat16 [16, 64, 2048], P('tp'), may hold values from -0.1875 to 0.1875
- ffn_gain: float32 [2048], replicated, may hold values from 0.1 to 1.9
- expert_gate: bfloat16 [256, 2048, 512], P(('ep', 'tp')), may hold values from -0.125 to 0.125
- expert_up: bfloat16 [256, 2048, 512], P(('ep', 'tp')), may hold values from -0.125 to 0.125
- expert_down: bfloat16 [256, 512, 2048], P(('ep', 'tp')), may hold values from -0.25 to 0.25
- shared_gate: bfloat16 [2048, 512], P(None, 'tp'), may hold values from -0.125 to 0.125
- shared_up: bfloat16 [2048, 512], P(None, 'tp'), may hold values from -0.125 to 0.125
- shared_down: bfloat16 [512, 2048], P('tp'), may hold values from -0.25 to 0.25
- dense_gate: bfloat16 [2048, 1024], P(None, 'tp'), may hold values from -0.125 to 0.125
- dense_up: bfloat16 [2048, 1024], P(None, 'tp'), may hold values from -0.125 to 0.125
- dense_down: bfloat16 [1024, 2048], P('tp'), may hold values from -0.1875 to 0.1875
- branch_gate: bfloat16 [2048], replicated, may hold values from -0.125 to 0.125
Outputs:
- mixed: bfloat16 [1024, 2048], P(('ep', 'tp'))
- new_latent: bfloat16 [1024, 512], P(('ep', 'tp'))
- new_rope_key: bfloat16 [1024, 32], P(('ep', 'tp'))
The draws below stay inside these ranges and needn't reach their ends.
Inputs may be any that keep to these rules, and one draw needn't show every extreme that they name: `route_ids`: in each aligned block of 64 rows, no expert is named by more than 2 of the block's rows, a bound that some block reaches. Each row names 4 different experts.
All inputs are finite; a program needn't handle non-finite values.
Results may differ from the reference program's by a relative error of at most 0.025.
Values may be sent and summed in bfloat16 or wider, within the bound.
A program may use at most 64 MiB of HBM per device.

```python
import math
import jax
import jax.numpy as jnp
import numpy as np
from jax import lax

D = 2048
HEADS = 16
NOPE = 64
ROPE = 32
VHEAD = 64
LATENT = 512
EXPERT_FF = 512
SHARED_FF = 512
DENSE_FF = 1024
TOP_K = 4
LEN = 1024
GROUP = 64
SEQS = 1024
EXPERTS = 256
CAP = 2
N_EP = 16


def draw_cache_rope_key(key, part):
    values = jnp.clip(jax.random.normal(key, (SEQS, LEN, ROPE), jnp.float32), -6.0, 6.0)
    return values.astype(jnp.bfloat16)


def plant(array, rng, low, top_value):
    longest = array.shape.index(max(array.shape))
    spots = []
    for shift in (0, 1):
        where = [jax.random.randint(jax.random.fold_in(rng, axis), (), 0, length) for axis, length in enumerate(array.shape)]
        where[longest] = (where[longest] + shift) % array.shape[longest]
        spots.append(tuple(where))
    return array.at[spots[0]].set(low).at[spots[1]].set(top_value)


def steps_of(own_key, dims, cuts, low, high):
    gain, own = 1.0, jax.random.fold_in(own_key, 6)
    for axis_at, blocks in cuts:
        heights = jnp.exp(jax.random.uniform(jax.random.fold_in(own, axis_at), (blocks,), jnp.float32, low / len(cuts), high / len(cuts)))
        gain = gain * jnp.repeat(heights, dims[axis_at] // blocks).reshape([-1 if axis == axis_at else 1 for axis in range(len(dims))])
    return gain


def assign_block(rng, own, number, rows, number_of, top, most, skew):
    ranking = jax.random.permutation(rng, number_of)
    packed, common = load_shares(number_of, rows * top, most, skew, True), load_shares(number_of, rows * top, most, skew, False)
    places = jnp.arange(number_of)

    def named(sizes, rotation):
        used = int((sizes > 0).sum())
        fixed = max(1, used // 4)
        moved = fixed + (places - fixed + rotation * (used - fixed)) % max(1, number_of - fixed)
        return jnp.zeros((number_of,), jnp.int32).at[ranking[jnp.where(places < fixed, places, moved)]].set(jnp.asarray(sizes, jnp.int32))

    sizes = jnp.where(number % 4 == 0, named(packed, number // 4), named(common, number - number // 4 - 1))
    mixed = jax.random.permutation(jax.random.fold_in(own, 3), number_of)
    source_of, taker = mixed[0:number_of // 2 * 2:2], mixed[1:number_of // 2 * 2:2]
    slack = jnp.minimum(sizes[source_of] - 1, most - sizes[taker]) // 2
    slack = jnp.where((source_of == ranking[0]) | (taker == ranking[0]) | (sizes[taker] == 0), 0, jnp.maximum(slack, 0))
    moved = jax.random.randint(jax.random.fold_in(own, 4), (number_of // 2,), 0, 1 << 20) % (slack + 1)
    sizes = sizes.at[source_of].add(-moved).at[taker].add(moved)
    members = jnp.searchsorted(jnp.cumsum(sizes), jnp.arange(rows * top), side="right").astype(jnp.int32)
    grid = members.reshape(top, rows).T
    grid = grid[jax.random.permutation(jax.random.fold_in(own, 1), rows)]
    rotation = jax.random.randint(jax.random.fold_in(own, 2), (rows, 1), 0, top)
    return jnp.take_along_axis(grid, (jnp.arange(top)[None, :] + rotation) % top, axis=1)


def load_shares(count, total, most, slope, full):
    portions = [(1 << 20) // math.isqrt(rank ** slope) + 1 for rank in range(1, count + 1)]
    largest = most if full else min(most, max(-(-total // count), total * portions[0] // sum(portions)))
    least = 1 if total - largest >= count - 1 else 0
    given, rest = [largest] + [least] * (count - 1), total - largest - least * (count - 1)
    while rest > 0:
        candidates = [i for i in range(1, count) if given[i] < largest] or [i for i in range(1, count) if given[i] < most]
        pool, remaining = sum([portions[i] for i in candidates]), rest
        for i in candidates:
            addition = min(most - given[i], max(1, remaining * portions[i] // pool), rest)
            given[i] = given[i] + addition
            rest = rest - addition
    return np.array(given)


def bell_draw(own_key, shape, deviation, reach, pieces=(), held_as=jnp.bfloat16):
    level = steps_of(own_key, shape, pieces, -0.22, 0.18) if pieces else 1.0
    entries = jax.random.normal(own_key, shape, jnp.float32) * deviation * level
    return jnp.minimum(jnp.maximum(entries, -reach), reach).astype(held_as)


def setup_inputs(seed: int = 0) -> dict:
    key_list = jax.random.split(jax.random.key(seed), 27)
    tokens = bell_draw(key_list[0], (SEQS, D), 1.0, 6.0, ((0, 256),))
    lengths = plant(jax.random.randint(key_list[1], (SEQS,), LEN // 16, LEN + 1), jax.random.fold_in(key_list[1], 1), LEN // 16, LEN).astype(jnp.int32)
    cache_latent = bell_draw(key_list[2], (SEQS, LEN, LATENT), 1.0, 6.0, ((0, 256),))
    cache_rope_key = draw_cache_rope_key(jax.random.fold_in(key_list[26], 71), 0)
    route_ids_keys = jax.random.split(jax.random.fold_in(key_list[4], 1), SEQS // GROUP)
    route_ids_turns = jax.random.permutation(jax.random.fold_in(key_list[4], 3), SEQS // GROUP)
    route_ids = jax.vmap(lambda own, number: assign_block(jax.random.fold_in(key_list[4], 2), own, number, GROUP, EXPERTS, TOP_K, CAP, 2))(route_ids_keys, route_ids_turns).reshape((SEQS, TOP_K))
    route_weights = jnp.clip(jnp.exp(math.log(2.0) - 2.3025851 * jax.random.uniform(key_list[5], (SEQS, TOP_K), jnp.float32) ** steps_of(key_list[5], (SEQS, TOP_K), ((0, 16),), -0.2, 0.2)), 0.2, 2.0)
    attn_gain = jnp.clip(1.0 + 0.18 * jax.random.normal(key_list[6], (D,), jnp.float32), 0.1, 1.9)
    w_query_nope = bell_draw(key_list[7], (D, HEADS, NOPE), D ** -0.5, 0.125, ((1, 16),))
    w_query_rope = bell_draw(key_list[8], (D, HEADS, ROPE), D ** -0.5, 0.125, ((1, 16),))
    w_latent_down = bell_draw(key_list[9], (D, LATENT), D ** -0.5, 0.125, ((1, 16),))
    w_key_rope = bell_draw(key_list[10], (D, ROPE), D ** -0.5, 0.125)
    latent_gain = jnp.clip(1.0 + 0.18 * jax.random.normal(key_list[11], (LATENT,), jnp.float32), 0.1, 1.9)
    w_key_up = bell_draw(key_list[12], (LATENT, HEADS, NOPE), NOPE ** -0.5, 0.75, ((1, 16),))
    w_value_up = bell_draw(key_list[13], (LATENT, HEADS, VHEAD), LATENT ** -0.5, 0.25, ((1, 16),))
    w_attn_out = bell_draw(key_list[14], (HEADS, VHEAD, D), (HEADS * VHEAD) ** -0.5, 0.1875, ((0, 16),))
    ffn_gain = jnp.clip(1.0 + 0.18 * jax.random.normal(key_list[15], (D,), jnp.float32), 0.1, 1.9)
    expert_gate = bell_draw(key_list[16], (EXPERTS, D, EXPERT_FF), D ** -0.5, 0.125, ((0, 256),))
    expert_up = bell_draw(key_list[17], (EXPERTS, D, EXPERT_FF), D ** -0.5, 0.125, ((0, 256),))
    expert_down = bell_draw(key_list[18], (EXPERTS, EXPERT_FF, D), EXPERT_FF ** -0.5, 0.25, ((0, 256),))
    shared_gate = bell_draw(key_list[19], (D, SHARED_FF), D ** -0.5, 0.125, ((1, 16),))
    shared_up = bell_draw(key_list[20], (D, SHARED_FF), D ** -0.5, 0.125, ((1, 16),))
    shared_down = bell_draw(key_list[21], (SHARED_FF, D), SHARED_FF ** -0.5, 0.25, ((0, 16),))
    dense_gate = bell_draw(key_list[22], (D, DENSE_FF), D ** -0.5, 0.125, ((1, 16),))
    dense_up = bell_draw(key_list[23], (D, DENSE_FF), D ** -0.5, 0.125, ((1, 16),))
    dense_down = bell_draw(key_list[24], (DENSE_FF, D), DENSE_FF ** -0.5, 0.1875, ((0, 16),))
    branch_gate = bell_draw(key_list[25], (D,), D ** -0.5, 0.125)
    return dict(tokens=tokens, lengths=lengths, cache_latent=cache_latent, cache_rope_key=cache_rope_key, route_ids=route_ids, route_weights=route_weights, attn_gain=attn_gain, w_query_nope=w_query_nope, w_query_rope=w_query_rope, w_latent_down=w_latent_down, w_key_rope=w_key_rope, latent_gain=latent_gain, w_key_up=w_key_up, w_value_up=w_value_up, w_attn_out=w_attn_out, ffn_gain=ffn_gain, expert_gate=expert_gate, expert_up=expert_up, expert_down=expert_down, shared_gate=shared_gate, shared_up=shared_up, shared_down=shared_down, dense_gate=dense_gate, dense_up=dense_up, dense_down=dense_down, branch_gate=branch_gate)


epsilon = 1e-06
rope_base = 10000.0

def norm_rows(values, scales):
    values = values.astype(jnp.float32)
    factor = lax.rsqrt(lax.optimization_barrier(jnp.mean(values * values, axis=-1, keepdims=True)) + epsilon)
    return values * factor * scales.astype(jnp.float32)

def rotate(values, positions):
    half_dim = values.shape[-1] // 2
    frequencies = rope_base ** (-jnp.arange(half_dim).astype(jnp.float32) / half_dim)
    angles = positions.astype(jnp.float32)[:, None] * frequencies[None, :]
    bcast_shape = (angles.shape[0],) + (1,) * (values.ndim - 2) + (half_dim,)
    cosine = jnp.cos(angles).reshape(bcast_shape)
    sine_val = jnp.sin(angles).reshape(bcast_shape)
    first_half = values[..., :half_dim].astype(jnp.float32)
    second_half = values[..., half_dim:].astype(jnp.float32)
    return jnp.concatenate([first_half * cosine - second_half * sine_val, first_half * sine_val + second_half * cosine], axis=-1)

def swiglu(inputs, gate_w, up_w):
    gate_val = jnp.dot(inputs, gate_w, preferred_element_type=jnp.float32)
    up_val = jnp.dot(inputs, up_w, preferred_element_type=jnp.float32)
    return (jax.nn.silu(gate_val) * up_val).astype(jnp.bfloat16)

def attend(group_data):
    q_lat, q_rot, lat_new, rope_new, lat_cache, rope_cache, seq_len = group_data
    head_scale = (NOPE + ROPE) ** (-0.5)
    scores = jnp.einsum('bhr,blr->bhl', q_lat.astype(jnp.float32), lat_cache.astype(jnp.float32))
    scores = scores + jnp.einsum('bhe,ble->bhl', q_rot.astype(jnp.float32), rope_cache.astype(jnp.float32))
    scores = scores * head_scale
    in_range = jnp.arange(lat_cache.shape[1], dtype=jnp.int32)[None, None, :] < seq_len[:, None, None]
    scores = jnp.where(in_range, scores, -jnp.inf)
    own_score = jnp.einsum('bhr,br->bh', q_lat.astype(jnp.float32), lat_new.astype(jnp.float32))
    own_score = (own_score + jnp.einsum('bhe,be->bh', q_rot.astype(jnp.float32), rope_new.astype(jnp.float32))) * head_scale
    peak_score = jnp.maximum(lax.optimization_barrier(jnp.max(scores, axis=-1)), own_score)
    past_exp = jnp.exp(scores - peak_score[..., None])
    own_exp = jnp.exp(own_score - peak_score)
    total_exp = lax.optimization_barrier(jnp.sum(past_exp, axis=-1)) + own_exp
    past_weight = (past_exp / total_exp[..., None]).astype(jnp.bfloat16)
    own_weight = (own_exp / total_exp).astype(jnp.bfloat16)
    out_latent = jnp.einsum('bhl,blr->bhr', past_weight.astype(jnp.float32), lat_cache.astype(jnp.float32))
    out_latent = out_latent + own_weight.astype(jnp.float32)[..., None] * lat_new.astype(jnp.float32)[:, None, :]
    return out_latent.astype(jnp.bfloat16)

def reference(tokens, lengths, cache_latent, cache_rope_key, route_ids, route_weights, attn_gain, w_query_nope, w_query_rope, w_latent_down, w_key_rope, latent_gain, w_key_up, w_value_up, w_attn_out, ffn_gain, expert_gate, expert_up, expert_down, shared_gate, shared_up, shared_down, dense_gate, dense_up, dense_down, branch_gate):
    seq_count, model_width = tokens.shape
    head_count = w_query_nope.shape[1]
    normed = norm_rows(tokens, attn_gain).astype(jnp.bfloat16)
    query_nope = jnp.dot(normed, w_query_nope.reshape(model_width, -1), preferred_element_type=jnp.float32)
    query_nope = query_nope.astype(jnp.bfloat16).reshape(seq_count, head_count, -1)
    query_latent = jnp.einsum('shn,rhn->shr', query_nope.astype(jnp.float32), w_key_up.astype(jnp.float32)).astype(jnp.bfloat16)
    query_rope = jnp.dot(normed, w_query_rope.reshape(model_width, -1), preferred_element_type=jnp.float32)
    query_rope = query_rope.astype(jnp.bfloat16).reshape(seq_count, head_count, -1)
    latent_raw = jnp.dot(normed, w_latent_down, preferred_element_type=jnp.float32).astype(jnp.bfloat16)
    new_latent = norm_rows(latent_raw, latent_gain).astype(jnp.bfloat16)
    new_rope = rotate(jnp.dot(normed, w_key_rope, preferred_element_type=jnp.float32), lengths).astype(jnp.bfloat16)
    query_rot = rotate(query_rope, lengths).astype(jnp.bfloat16)
    grouped = tuple((member.reshape((N_EP, GROUP) + member.shape[1:]) for member in (query_latent, query_rot, new_latent, new_rope, cache_latent, cache_rope_key, lengths)))
    out_latent = lax.map(attend, grouped).reshape(seq_count, head_count, -1)
    head_values = jnp.einsum('shr,rhv->shv', out_latent.astype(jnp.float32), w_value_up.astype(jnp.float32)).astype(jnp.bfloat16)
    after_attn = tokens.astype(jnp.float32) + jnp.dot(head_values.reshape(seq_count, -1), w_attn_out.reshape(-1, model_width), preferred_element_type=jnp.float32)
    ffn_in = norm_rows(after_attn, ffn_gain).astype(jnp.bfloat16)
    shared_term = jnp.dot(swiglu(ffn_in, shared_gate, shared_up), shared_down, preferred_element_type=jnp.float32)
    branch_mix = jax.nn.sigmoid(jnp.dot(ffn_in, branch_gate, preferred_element_type=jnp.float32))
    dense_term = branch_mix[:, None] * jnp.dot(swiglu(ffn_in, dense_gate, dense_up), dense_down, preferred_element_type=jnp.float32)
    top_count = route_ids.shape[1]
    flat_expert = route_ids.reshape(-1).astype(jnp.int32)
    flat_row = jnp.arange(seq_count * top_count, dtype=jnp.int32) // top_count
    expert_hits = (flat_expert[:, None] == jnp.arange(EXPERTS, dtype=jnp.int32)[None, :]).astype(jnp.int32)
    expert_hits = expert_hits.reshape(N_EP, GROUP * top_count, EXPERTS)
    earlier = jnp.cumsum(expert_hits, axis=1) - expert_hits
    rank_in = lax.optimization_barrier(jnp.sum(earlier * expert_hits, axis=2)).reshape(-1).astype(jnp.int32)
    slot_index = (flat_row // GROUP * CAP + rank_in).astype(jnp.int32)
    slot_table = jnp.full((EXPERTS, N_EP * CAP), seq_count, jnp.int32).at[flat_expert, slot_index].set(flat_row)
    padded_in = jnp.concatenate([ffn_in, jnp.zeros((1, model_width), jnp.bfloat16)], axis=0)

    def one_expert(expert_data):
        row_ids, gate_w, up_w, down_w = expert_data
        act_val = swiglu(padded_in[row_ids], gate_w, up_w)
        return jnp.dot(act_val, down_w, preferred_element_type=jnp.float32).astype(jnp.bfloat16)
    expert_out = lax.map(one_expert, (slot_table, expert_gate, expert_up, expert_down))
    picked = expert_out[flat_expert, slot_index].astype(jnp.float32).reshape(seq_count, top_count, model_width)
    routed = lax.optimization_barrier(jnp.sum(picked * route_weights.astype(jnp.float32)[:, :, None], axis=1))
    mixed = (after_attn + routed + shared_term + dense_term).astype(jnp.bfloat16)
    return (mixed, new_latent, new_rope)
```

```python
import functools

import jax
import jax.numpy as jnp
from jax import lax
from jax.experimental import pallas as pl
from jax.experimental.pallas import tpu as pltpu
from jax.sharding import PartitionSpec as P

EPS = 1e-06
ROPE_BASE = 10000.0
MESH = pl.DeviceIdType.MESH
F32 = jnp.float32
BF16 = jnp.bfloat16


def nn(a, b):
    return lax.dot_general(a, b, (((1,), (0,)), ((), ())), preferred_element_type=F32)


def nt(a, b):
    return lax.dot_general(a, b, (((1,), (1,)), ((), ())), preferred_element_type=F32)


def tn(a, b):
    return lax.dot_general(a, b, (((0,), (0,)), ((), ())), preferred_element_type=F32)


def normed_rows(x, gain):
    return x * lax.rsqrt(jnp.mean(x * x, axis=-1, keepdims=True) + EPS) * gain


def silu(v):
    return v / (1.0 + jnp.exp(-v))


def layer_kernel(
    n_tp,
    n_ep,
    lengths,
    tokens,
    cache_h,
    rope_h,
    ids_h,
    rw_h,
    again_h,
    wqn_h,
    wqr_h,
    wld_h,
    wkr_h,
    lgain_h,
    wku_h,
    wvu_h,
    wao_h,
    fgain_h,
    eg_h,
    eu_h,
    ed_h,
    sg_h,
    su_h,
    sd_h,
    dg_h,
    du_h,
    dd_h,
    bg_h,
    mixed_o,
    nlat_o,
    nrope_o,
    cache,
    rope,
    ids,
    rw,
    again,
    w1,
    wkr,
    lgain,
    wku,
    wvu,
    wao,
    fgain,
    eg,
    eu,
    ed,
    w2,
    sd,
    dd,
    bg,
    xa,
    bs,
    br,
    cs,
    cr,
    ds_,
    dr,
    ee,
    fs,
    fr,
    gs,
    gr,
    hs,
    hr,
    big,
    small,
    rf,
    krs,
    lsem,
    send,
    recv,
):
    me = lax.axis_index("tp")
    grp = lax.axis_index("ep")
    rows, width = tokens.shape
    group = rows * n_tp
    nope = wqn_h.shape[0]
    ropew = wqr_h.shape[0]
    latw = wld_h.shape[0]
    latent = wku_h.shape[1]
    length = cache.shape[1]
    scale = (nope + ropew) ** (-0.5)

    wide = latent + 128

    def put(where, value):
        for k in range(value.shape[1] // 128):
            rf[k, where, :] = value[:, 128 * k : 128 * k + 128]

    def get(where, columns):
        return jnp.concatenate([rf[k, where, :] for k in range(columns // 128)], axis=1)

    jobs = [
        (tokens, xa.at[me]),
        (again_h, again),
        (wqn_h, w1.at[pl.ds(0, nope)]),
        (wqr_h, w1.at[pl.ds(nope, ropew)]),
        (wld_h, w1.at[pl.ds(nope + ropew, latw)]),
        (wkr_h, wkr),
        (wku_h, wku),
        (lgain_h, lgain),
        (cache_h, cache),
        (rope_h, rope),
        (wvu_h, wvu),
        (wao_h, wao),
        (fgain_h, fgain),
        (ids_h, ids),
        (rw_h, rw),
        (bg_h, bg),
        (sg_h, w2.at[pl.ds(0, sg_h.shape[0])]),
        (su_h, w2.at[pl.ds(sg_h.shape[0], sg_h.shape[0])]),
        (dg_h, w2.at[pl.ds(2 * sg_h.shape[0], dg_h.shape[0])]),
        (du_h, w2.at[pl.ds(2 * sg_h.shape[0] + dg_h.shape[0], dg_h.shape[0])]),
        (eg_h, eg),
        (eu_h, eu),
        (ed_h, ed),
        (sd_h, sd),
        (dd_h, dd),
    ]
    local = [pltpu.make_async_copy(s, d, lsem.at[i]) for i, (s, d) in enumerate(jobs)]
    for c in local:
        c.start()

    barrier = pltpu.get_barrier_semaphore()

    def greet(i, _):
        pl.semaphore_signal(
            barrier, inc=1, device_id={"tp": lax.rem(me + i, n_tp)}, device_id_type=MESH
        )
        return 0

    def greet_ep(i, _):
        pl.semaphore_signal(
            barrier, inc=1, device_id={"ep": lax.rem(grp + i, n_ep)}, device_id_type=MESH
        )
        return 0

    lax.fori_loop(1, n_tp, greet, 0)
    lax.fori_loop(1, n_ep, greet_ep, 0)

    def hop(phase, i, axis, n, mine, src, dst):
        to = lax.rem(mine + i, n)
        return pltpu.make_async_remote_copy(
            src_ref=src(to),
            dst_ref=dst.at[mine],
            send_sem=send.at[phase, i],
            recv_sem=recv.at[phase, i],
            device_id={axis: to},
            device_id_type=MESH,
        )

    def start_all(phase, axis, n, mine, src, dst):
        def body(i, _):
            hop(phase, i, axis, n, mine, src, dst).start()
            return 0

        lax.fori_loop(1, n, body, 0)

    def wait_all(phase, axis, n, mine, src, dst):
        def body(i, _):
            hop(phase, i, axis, n, mine, src, dst).wait_recv()
            return 0

        lax.fori_loop(1, n, body, 0)

    def wait_sent(phase, axis, n, mine, src, dst):
        def body(i, _):
            hop(phase, i, axis, n, mine, src, dst).wait_send()
            return 0

        lax.fori_loop(1, n, body, 0)

    ex = [
        (0, "tp", n_tp, me, lambda to: xa.at[me], xa),
        (1, "tp", n_tp, me, lambda to: bs.at[to], br),
        (2, "tp", n_tp, me, lambda to: cs.at[to], cr),
        (3, "tp", n_tp, me, lambda to: ds_.at[to], dr),
        (4, "tp", n_tp, me, lambda to: ee.at[me], ee),
        (5, "ep", n_ep, grp, lambda to: fs.at[to], fr),
        (6, "ep", n_ep, grp, lambda to: gs.at[to], gr),
        (7, "tp", n_tp, me, lambda to: hs.at[to], hr),
    ]

    lane = lax.broadcasted_iota(jnp.int32, (rows, 128), 1)
    rowi = lax.broadcasted_iota(jnp.int32, (rows, 128), 0)
    half = ropew // 2
    freq = jnp.zeros((rows, 128), F32)
    for i in range(half):
        freq = jnp.where(lane % half == i, F32(ROPE_BASE ** (-i / half)), freq)
    pos = jnp.zeros((rows, 128), jnp.int32)
    for s in range(rows):
        pos = jnp.where(rowi == s, lengths[s], pos)
    angle = pos.astype(F32) * freq
    cosv = jnp.cos(angle)
    sinv = jnp.sin(angle)

    def rotated(v, c, s):
        ln = lax.broadcasted_iota(jnp.int32, v.shape, 1)
        other = jnp.where(
            ln % ropew < half, -pltpu.roll(v, 128 - half, 1), pltpu.roll(v, half, 1)
        )
        return v * c + other * s

    pl.semaphore_wait(barrier, (n_tp - 1) + (n_ep - 1))
    local[0].wait()
    start_all(*ex[0])

    local[1].wait()
    local[5].wait()
    tok = xa[me].astype(F32)
    own_normed = normed_rows(tok, again[...]).astype(BF16)
    krs[...] = jnp.zeros_like(krs)
    krs[:, 0:ropew] = nt(own_normed, wkr[...])
    new_rope = rotated(krs[...], cosv, sinv).astype(BF16).astype(F32)
    nrope_o[...] = new_rope[:, 0:ropew].astype(BF16)
    for i in (2, 3, 4, 6, 7):
        local[i].wait()

    wait_all(*ex[0])
    for t in range(n_tp):
        big[pl.ds(rows * t, rows), :] = xa[t].astype(F32)
    normed = normed_rows(big[...], again[...]).astype(BF16)
    y = nt(normed, w1[...])
    ql = nn(y[:, 0:nope].astype(BF16), wku[...])
    put(pl.ds(0, group), jnp.concatenate([ql, y], axis=1))
    for t in range(n_tp):
        bs[t] = get(pl.ds(rows * t, rows), wide).astype(BF16)
    start_all(*ex[1])
    br[me] = bs[me]
    wait_all(*ex[1])
    for t in range(n_tp):
        put(pl.ds(rows * t, rows), br[t].astype(F32))

    parts = []
    ln4 = lax.broadcasted_iota(jnp.int32, (rows, 128), 1)
    per = 128 // latw
    for k in range(latent // 128):
        acc = jnp.zeros((rows, 128), F32)
        for j in range(per):
            piece = br[k * per + j][:, latent : latent + 128].astype(F32)
            shift = (j * latw - (nope + ropew)) % 128
            if shift:
                piece = pltpu.roll(piece, shift, 1)
            acc = jnp.where(ln4 // latw == j, piece, acc)
        parts.append(acc)
    latent_raw = jnp.concatenate(parts, axis=1)
    nl16 = normed_rows(latent_raw, lgain[...]).astype(BF16)
    nlat_o[...] = nl16
    new_latent = nl16.astype(F32)
    lane_r = lax.broadcasted_iota(jnp.int32, (rows, 128), 1)
    nr_al = jnp.where(
        (lane_r >= nope) & (lane_r < nope + ropew), pltpu.roll(new_rope, nope, 1), 0.0
    )

    local[8].wait()
    local[9].wait()
    n_heads = n_tp
    outs = []
    for s in range(rows):
        q = get(pl.ds(s, n_heads, stride=rows), latent)
        qr = rf[latent // 128, pl.ds(s, n_heads, stride=rows), :]
        qrot = rotated(qr, cosv[s : s + 1], sinv[s : s + 1]).astype(BF16)
        sc = nt(q.astype(BF16), cache[s])
        sc = (sc + nn(qrot[:, nope : nope + ropew], rope[s])) * scale
        col = lax.broadcasted_iota(jnp.int32, (n_heads, length), 1)
        sc = jnp.where(col < lengths[s], sc, -jnp.inf)
        nls = new_latent[s : s + 1]
        own = (
            jnp.sum(q * nls, axis=-1, keepdims=True)
            + jnp.sum(qrot.astype(F32) * nr_al[s : s + 1], axis=-1, keepdims=True)
        ) * scale
        peak = jnp.maximum(jnp.max(sc, axis=-1, keepdims=True), own)
        pe = jnp.exp(sc - peak)
        oe = jnp.exp(own - peak)
        inv = 1.0 / (jnp.sum(pe, axis=-1, keepdims=True) + oe)
        pw = (pe * inv).astype(BF16)
        ow = (oe * inv).astype(BF16).astype(F32)
        outs.append(nn(pw, cache[s]) + ow * nls)
    for s in range(rows):
        put(pl.ds(s, n_heads, stride=rows), outs[s])
    for t in range(n_tp):
        cs[t] = get(pl.ds(rows * t, rows), latent).astype(BF16)
    start_all(*ex[2])
    cr[me] = cs[me]
    for i in range(10, 16):
        local[i].wait()

    cap = fs.shape[1]
    slots = n_ep * cap
    sl = lax.broadcasted_iota(jnp.int32, (slots, group), 0)
    want = (sl // cap) * n_tp + me
    hit = jnp.zeros((slots, group), F32)
    wgt = jnp.zeros((slots, group), F32)
    for k in range(ids_h.shape[0]):
        m = ids[k : k + 1, :] == want
        hit = jnp.where(m, 1.0, hit)
        wgt = jnp.where(m, rw[k : k + 1, :], wgt)
    before = (
        lax.broadcasted_iota(jnp.int32, (group, group), 0)
        < lax.broadcasted_iota(jnp.int32, (group, group), 1)
    )
    rank = nn(hit.astype(BF16), jnp.where(before, 1.0, 0.0).astype(BF16))
    taken = (hit > 0.5) & (jnp.abs(rank - (sl % cap).astype(F32)) < 0.5)
    disp = jnp.where(taken, 1.0, 0.0).astype(BF16)
    comb = jnp.where(taken, wgt, 0.0)
    comb_hi = comb.astype(BF16)
    comb_lo = (comb - comb_hi.astype(F32)).astype(BF16)

    wait_all(*ex[2])
    for t in range(n_tp):
        put(pl.ds(rows * t, rows), cr[t].astype(F32))
    hv = nt(get(pl.ds(0, group), latent).astype(BF16), wvu[...]).astype(BF16)
    big[...] = nn(hv, wao[...])
    for t in range(n_tp):
        ds_[t] = big[pl.ds(rows * t, rows), :].astype(BF16)
    start_all(*ex[3])
    dr[me] = ds_[me]
    for i in range(16, len(jobs)):
        local[i].wait()
    wait_all(*ex[3])
    after = tok
    total = jnp.zeros_like(tok)
    for t in range(n_tp):
        total = total + dr[t].astype(F32)
    after = tok + total
    ee[me] = normed_rows(after, fgain[...]).astype(BF16)
    start_all(*ex[4])
    wait_all(*ex[4])
    for t in range(n_tp):
        big[pl.ds(rows * t, rows), :] = ee[t].astype(F32)
    ffn = big[...].astype(BF16)
    out = nn(disp, ffn)
    mix = jax.nn.sigmoid(jnp.sum(big[...] * bg[...], axis=-1, keepdims=True))
    small[...] = out
    for g in range(n_ep):
        fs[g] = small[pl.ds(cap * g, cap), :].astype(BF16)
    start_all(*ex[5])
    fr[grp] = fs[grp]
    h = nt(ffn, w2[...])
    a, b = sg_h.shape[0], dg_h.shape[0]
    sact = (silu(h[:, 0:a]) * h[:, a : 2 * a]).astype(BF16)
    dact = (silu(h[:, 2 * a : 2 * a + b]) * h[:, 2 * a + b : 2 * a + 2 * b]).astype(BF16)
    wait_all(*ex[5])
    for g in range(n_ep):
        small[pl.ds(cap * g, cap), :] = fr[g].astype(F32)
    arrived = small[...].astype(BF16)
    act = (silu(nn(arrived, eg[...])) * nn(arrived, eu[...])).astype(BF16)
    small[...] = nn(act, ed[...])
    for g in range(n_ep):
        gs[g] = small[pl.ds(cap * g, cap), :].astype(BF16)
    start_all(*ex[6])
    gr[grp] = gs[grp]
    big[...] = nn(sact, sd[...]) + mix * nn(dact, dd[...])
    wait_all(*ex[6])
    for g in range(n_ep):
        small[pl.ds(cap * g, cap), :] = gr[g].astype(F32)
    back = small[...].astype(BF16)
    big[...] += tn(comb_hi, back) + tn(comb_lo, back)
    for t in range(n_tp):
        hs[t] = big[pl.ds(rows * t, rows), :].astype(BF16)
    start_all(*ex[7])
    hr[me] = hs[me]
    for e in ex[:7]:
        wait_sent(*e)
    wait_all(*ex[7])
    total = jnp.zeros_like(tok)
    for t in range(n_tp):
        total = total + hr[t].astype(F32)
    mixed_o[...] = (after + total).astype(BF16)
    wait_sent(*ex[7])


def local(
    tokens,
    lengths,
    cache_latent,
    cache_rope_key,
    route_ids,
    route_weights,
    attn_gain,
    w_query_nope,
    w_query_rope,
    w_latent_down,
    w_key_rope,
    latent_gain,
    w_key_up,
    w_value_up,
    w_attn_out,
    ffn_gain,
    expert_gate,
    expert_up,
    expert_down,
    shared_gate,
    shared_up,
    shared_down,
    dense_gate,
    dense_up,
    dense_down,
    branch_gate,
):
    n_tp = lax.axis_size("tp")
    n_ep = lax.axis_size("ep")
    rows, width = tokens.shape
    group = rows * n_tp
    wqn = w_query_nope.reshape(width, -1).T
    wqr = w_query_rope.reshape(width, -1).T
    wld = w_latent_down.T
    wkr = w_key_rope.T
    wku = w_key_up.reshape(w_key_up.shape[0], -1).T
    wvu = w_value_up.reshape(w_value_up.shape[0], -1).T
    wao = w_attn_out.reshape(-1, width)
    sg, su, dg, du = shared_gate.T, shared_up.T, dense_gate.T, dense_up.T
    rope = jnp.swapaxes(cache_rope_key, 1, 2)
    latent = wku.shape[1]
    ropew = wqr.shape[0]
    cap = max(2, -(-2 * rows * route_ids.shape[1] // n_ep))
    args = [
        lengths,
        tokens,
        cache_latent,
        rope,
        route_ids.T,
        route_weights.T,
        attn_gain.reshape(1, -1),
        wqn,
        wqr,
        wld,
        wkr,
        latent_gain.reshape(1, -1),
        wku,
        wvu,
        wao,
        ffn_gain.reshape(1, -1),
        expert_gate[0],
        expert_up[0],
        expert_down[0],
        sg,
        su,
        shared_down,
        dg,
        du,
        dense_down,
        branch_gate.astype(F32).reshape(1, -1),
    ]
    any_spec = pl.BlockSpec(memory_space=pl.ANY)
    vm = lambda a: pltpu.VMEM(a.shape, a.dtype)
    n1 = wqn.shape[0] + ropew + wld.shape[0]
    n2 = 2 * (sg.shape[0] + dg.shape[0])
    wide = latent + 128
    scratch = [
        vm(cache_latent),
        vm(rope),
        vm(args[4]),
        vm(args[5]),
        vm(args[6]),
        pltpu.VMEM((n1, width), BF16),
        vm(wkr),
        vm(args[11]),
        vm(wku),
        vm(wvu),
        vm(wao),
        vm(args[15]),
        vm(args[16]),
        vm(args[17]),
        vm(args[18]),
        pltpu.VMEM((n2, width), BF16),
        vm(shared_down),
        vm(dense_down),
        vm(args[25]),
        pltpu.VMEM((n_tp, rows, width), BF16),
        pltpu.VMEM((n_tp, rows, wide), BF16),
        pltpu.VMEM((n_tp, rows, wide), BF16),
        pltpu.VMEM((n_tp, rows, latent), BF16),
        pltpu.VMEM((n_tp, rows, latent), BF16),
        pltpu.VMEM((n_tp, rows, width), BF16),
        pltpu.VMEM((n_tp, rows, width), BF16),
        pltpu.VMEM((n_tp, rows, width), BF16),
        pltpu.VMEM((n_ep, cap, width), BF16),
        pltpu.VMEM((n_ep, cap, width), BF16),
        pltpu.VMEM((n_ep, cap, width), BF16),
        pltpu.VMEM((n_ep, cap, width), BF16),
        pltpu.VMEM((n_tp, rows, width), BF16),
        pltpu.VMEM((n_tp, rows, width), BF16),
        pltpu.VMEM((group, width), F32),
        pltpu.VMEM((n_ep * cap, width), F32),
        pltpu.VMEM((wide // 128, group, 128), F32),
        pltpu.VMEM((rows, 128), F32),
        pltpu.SemaphoreType.DMA((25,)),
        pltpu.SemaphoreType.DMA((8, max(n_tp, n_ep))),
        pltpu.SemaphoreType.DMA((8, max(n_tp, n_ep))),
    ]
    return pl.pallas_call(
        functools.partial(layer_kernel, n_tp, n_ep),
        out_shape=(
            jax.ShapeDtypeStruct((rows, width), BF16),
            jax.ShapeDtypeStruct((rows, latent), BF16),
            jax.ShapeDtypeStruct((rows, ropew), BF16),
        ),
        in_specs=[pl.BlockSpec(memory_space=pltpu.SMEM)] + [any_spec] * 25,
        out_specs=(pl.BlockSpec(memory_space=pltpu.VMEM),) * 3,
        scratch_shapes=scratch,
        compiler_params=pltpu.CompilerParams(
            collective_id=0, has_side_effects=True, vmem_limit_bytes=56 * 1024 * 1024
        ),
        name="layer",
    )(*args)


def solution(mesh):
    in_specs = (
        P(("ep", "tp"), None),
        P(("ep", "tp")),
        P(("ep", "tp"), None, None),
        P(("ep", "tp"), None, None),
        P("ep", None),
        P("ep", None),
        P(),
        P(None, "tp", None),
        P(None, "tp", None),
        P(None, "tp"),
        P(),
        P(),
        P(None, "tp", None),
        P(None, "tp", None),
        P("tp", None, None),
        P(),
        P(("ep", "tp"), None, None),
        P(("ep", "tp"), None, None),
        P(("ep", "tp"), None, None),
        P(None, "tp"),
        P(None, "tp"),
        P("tp", None),
        P(None, "tp"),
        P(None, "tp"),
        P("tp", None),
        P(),
    )
    out_specs = (P(("ep", "tp"), None), P(("ep", "tp"), None), P(("ep", "tp"), None))
    return jax.shard_map(local, mesh=mesh, in_specs=in_specs, out_specs=out_specs, check_vma=False)
```

```python
import functools

import jax
import jax.numpy as jnp
from jax import lax
from jax.experimental import pallas as pl
from jax.experimental.pallas import tpu as pltpu
from jax.sharding import PartitionSpec as P

EPS = 1e-06
ROPE_BASE = 10000.0
MESH = pl.DeviceIdType.MESH
F32 = jnp.float32
BF16 = jnp.bfloat16


def nn(a, b):
    return lax.dot_general(a, b, (((1,), (0,)), ((), ())), preferred_element_type=F32)


def nt(a, b):
    return lax.dot_general(a, b, (((1,), (1,)), ((), ())), preferred_element_type=F32)


def tn(a, b):
    return lax.dot_general(a, b, (((0,), (0,)), ((), ())), preferred_element_type=F32)


def normed_rows(x, gain):
    return x * lax.rsqrt(jnp.mean(x * x, axis=-1, keepdims=True) + EPS) * gain


def silu(v):
    return v / (1.0 + jnp.exp(-v))


def finish_kernel(mixed, nlat, nrope, mixed_o, nlat_o, nrope_o):
    mixed_o[...] = mixed[...]
    nlat_o[...] = nlat[...]
    nrope_o[...] = nrope[...]


def layer_kernel(
    n_tp,
    n_ep,
    lengths,
    tokens,
    cache_h,
    rope_h,
    ids_h,
    rw_h,
    again_h,
    wqn_h,
    wqr_h,
    wld_h,
    wkr_h,
    lgain_h,
    wku_h,
    wvu_h,
    wao_h,
    fgain_h,
    eg_h,
    eu_h,
    ed_h,
    sg_h,
    su_h,
    sd_h,
    dg_h,
    du_h,
    dd_h,
    bg_h,
    mixed_o,
    nlat_o,
    nrope_o,
    cache,
    rope,
    ids,
    rw,
    again,
    w1,
    wkr,
    lgain,
    wku,
    wvu,
    wao,
    fgain,
    eg,
    eu,
    ed,
    w2,
    sd,
    dd,
    bg,
    xa,
    bs,
    br,
    cs,
    cr,
    ds_,
    dp,
    dm,
    dr,
    ee,
    fs,
    fr,
    gs,
    gr,
    hs,
    hp,
    hm,
    hr,
    qbd,
    big,
    small,
    rf,
    krs,
    lsem,
    send,
    recv,
):
    me = lax.axis_index("tp")
    grp = lax.axis_index("ep")
    rows, width = tokens.shape
    group = rows * n_tp
    nope = wqn_h.shape[0]
    ropew = wqr_h.shape[0]
    latw = wld_h.shape[0]
    latent = wku_h.shape[1]
    length = cache.shape[1]
    scale = (nope + ropew) ** (-0.5)

    wide = latent + 128
    n_z = n_tp // 2
    core = lax.rem(me, 2)
    place = lax.div(me, 2)

    def put(where, value):
        for k in range(value.shape[1] // 128):
            rf[k, where, :] = value[:, 128 * k : 128 * k + 128]

    def get(where, columns):
        return jnp.concatenate([rf[k, where, :] for k in range(columns // 128)], axis=1)

    jobs = [
        (tokens, xa.at[core, place]),
        (again_h, again),
        (wqn_h, w1.at[pl.ds(0, nope)]),
        (wqr_h, w1.at[pl.ds(nope, ropew)]),
        (wld_h, w1.at[pl.ds(nope + ropew, latw)]),
        (wkr_h, wkr),
        (wku_h, wku),
        (lgain_h, lgain),
        (cache_h, cache),
        (rope_h, rope),
        (wvu_h, wvu),
        (wao_h, wao),
        (fgain_h, fgain),
        (ids_h, ids),
        (rw_h, rw),
        (bg_h, bg),
        (sg_h, w2.at[pl.ds(0, sg_h.shape[0])]),
        (su_h, w2.at[pl.ds(sg_h.shape[0], sg_h.shape[0])]),
        (dg_h, w2.at[pl.ds(2 * sg_h.shape[0], dg_h.shape[0])]),
        (du_h, w2.at[pl.ds(2 * sg_h.shape[0] + dg_h.shape[0], dg_h.shape[0])]),
        (eg_h, eg),
        (eu_h, eu),
        (ed_h, ed),
        (sd_h, sd),
        (dd_h, dd),
    ]
    local = [pltpu.make_async_copy(s, d, lsem.at[i]) for i, (s, d) in enumerate(jobs)]
    for c in local:
        c.start()

    barrier = pltpu.get_barrier_semaphore()

    def greet(i, _):
        pl.semaphore_signal(
            barrier, inc=1, device_id={"tp": lax.rem(me + i, n_tp)}, device_id_type=MESH
        )
        return 0

    def greet_ep(i, _):
        pl.semaphore_signal(
            barrier, inc=1, device_id={"ep": lax.rem(grp + i, n_ep)}, device_id_type=MESH
        )
        return 0

    lax.fori_loop(1, n_tp, greet, 0)
    lax.fori_loop(1, n_ep, greet_ep, 0)

    def hop(phase, axis, to, src, dst):
        return pltpu.make_async_remote_copy(
            src_ref=src,
            dst_ref=dst,
            send_sem=send.at[phase],
            recv_sem=recv.at[phase],
            device_id={axis: to},
            device_id_type=MESH,
        )

    def wait_bytes(sem, like):
        pltpu.make_async_copy(like, like, sem).wait()

    def to_all(phase, axis, n, mine, src, dst):
        def body(i, _):
            to = lax.rem(mine + n // 2 + i, n)

            @pl.when(to != mine)
            def _():
                hop(phase, axis, to, src.at[to], dst.at[mine]).start()

            return 0

        lax.fori_loop(0, n, body, 0)
        dst[mine] = src[mine]

    def await_all(phase, n, dst):
        wait_bytes(recv.at[phase], dst.at[pl.ds(0, n - 1)])

    def along_z(phase, pick, dst):
        def body(i, _):
            up = lax.rem(place + i, n_z)
            down = lax.rem(place + n_z - i, n_z)
            hop(phase, "tp", 2 * up + core, pick(up), dst).start()

            @pl.when(up != down)
            def _():
                hop(phase, "tp", 2 * down + core, pick(down), dst).start()

            return 0

        lax.fori_loop(0, n_z // 2, lambda j, x: body(n_z // 2 - j, x), 0)

    def gather(phase, buf):
        along_z(phase, lambda to: buf.at[core, place], buf.at[core, place])

    def gather_rest(phase, buf):
        wait_bytes(recv.at[phase], buf.at[0, pl.ds(0, n_z - 1)])
        hop(phase + 1, "tp", 2 * place + 1 - core, buf.at[core], buf.at[core]).start()
        wait_bytes(recv.at[phase + 1], buf.at[0])

    def reduce_start(phase, src, pair):
        hop(phase, "tp", 2 * place + 1 - core, src.at[1 - core], pair).start()

    def reduce_rest(phase, src, pair, mid, dst):
        wait_bytes(recv.at[phase], pair)
        for z in range(n_z):
            mid[z] = (src[core, z].astype(F32) + pair[z].astype(F32)).astype(BF16)
        along_z(phase + 1, lambda to: mid.at[to], dst.at[place])
        dst[place] = mid[place]

    def reduce_sum(phase, dst):
        wait_bytes(recv.at[phase + 1], dst.at[pl.ds(0, n_z - 1)])
        total = dst[0].astype(F32)
        for z in range(1, n_z):
            total = total + dst[z].astype(F32)
        return total

    lane = lax.broadcasted_iota(jnp.int32, (rows, 128), 1)
    rowi = lax.broadcasted_iota(jnp.int32, (rows, 128), 0)
    half = ropew // 2
    freq = jnp.zeros((rows, 128), F32)
    for i in range(half):
        freq = jnp.where(lane % half == i, F32(ROPE_BASE ** (-i / half)), freq)
    pos = jnp.zeros((rows, 128), jnp.int32)
    for s in range(rows):
        pos = jnp.where(rowi == s, lengths[s], pos)
    angle = pos.astype(F32) * freq
    cosv = jnp.cos(angle)
    sinv = jnp.sin(angle)

    def rotated(v, c, s):
        ln = lax.broadcasted_iota(jnp.int32, v.shape, 1)
        other = jnp.where(
            ln % ropew < half, -pltpu.roll(v, 128 - half, 1), pltpu.roll(v, half, 1)
        )
        return v * c + other * s

    pl.semaphore_wait(barrier, (n_tp - 1) + (n_ep - 1))
    local[0].wait()
    gather(0, xa)

    local[1].wait()
    local[5].wait()
    tok = xa[core, place].astype(F32)
    own_normed = normed_rows(tok, again[...]).astype(BF16)
    krs[...] = jnp.zeros_like(krs)
    qbd[...] = jnp.zeros_like(qbd)
    krs[:, 0:ropew] = nt(own_normed, wkr[...])
    new_rope = rotated(krs[...], cosv, sinv).astype(BF16).astype(F32)
    nrope_o[...] = new_rope[:, 0:ropew].astype(BF16)
    for i in (2, 3, 4, 6, 7):
        local[i].wait()

    gather_rest(0, xa)
    for t in range(n_tp):
        big[pl.ds(rows * t, rows), :] = xa[t % 2, t // 2].astype(F32)
    normed = normed_rows(big[...], again[...]).astype(BF16)
    y = nt(normed, w1[...])
    ql = nn(y[:, 0:nope].astype(BF16), wku[...])
    put(pl.ds(0, group), jnp.concatenate([ql, y], axis=1))
    for t in range(n_tp):
        bs[t] = get(pl.ds(rows * t, rows), wide).astype(BF16)
    to_all(2, "tp", n_tp, me, bs, br)
    await_all(2, n_tp, br)
    for t in range(n_tp):
        put(pl.ds(rows * t, rows), br[t].astype(F32))

    parts = []
    ln4 = lax.broadcasted_iota(jnp.int32, (rows, 128), 1)
    per = 128 // latw
    for k in range(latent // 128):
        acc = jnp.zeros((rows, 128), F32)
        for j in range(per):
            piece = br[k * per + j][:, latent : latent + 128].astype(F32)
            shift = (j * latw - (nope + ropew)) % 128
            if shift:
                piece = pltpu.roll(piece, shift, 1)
            acc = jnp.where(ln4 // latw == j, piece, acc)
        parts.append(acc)
    latent_raw = jnp.concatenate(parts, axis=1)
    nl16 = normed_rows(latent_raw, lgain[...]).astype(BF16)
    nlat_o[...] = nl16
    new_latent = nl16.astype(F32)
    lane_r = lax.broadcasted_iota(jnp.int32, (rows, 128), 1)
    nr_al = jnp.where(
        (lane_r >= nope) & (lane_r < nope + ropew), pltpu.roll(new_rope, nope, 1), 0.0
    )

    local[8].wait()
    local[9].wait()
    n_heads = n_tp
    pairs = rows * n_heads
    nlr = [new_latent[s : s + 1] for s in range(rows)]
    qrots, owns = [], []
    for s in range(rows):
        q = get(pl.ds(s, n_heads, stride=rows), latent)
        qr = rf[latent // 128, pl.ds(s, n_heads, stride=rows), :]
        qbd[pl.ds(n_heads * s, n_heads), latent * s : latent * (s + 1)] = q.astype(BF16)
        qrot = rotated(qr, cosv[s : s + 1], sinv[s : s + 1]).astype(BF16).astype(F32)
        owns.append(
            (
                jnp.sum(q * nlr[s], axis=-1, keepdims=True)
                + jnp.sum(qrot * nr_al[s : s + 1], axis=-1, keepdims=True)
            )
            * scale
        )
        shift = (ropew * s - nope) % 128
        lnq = lax.broadcasted_iota(jnp.int32, qrot.shape, 1)
        qrots.append(
            jnp.where(lnq // ropew == s, pltpu.roll(qrot, shift, 1) if shift else qrot, 0.0)
        )
    qrbd = jnp.concatenate(qrots, axis=0).astype(BF16)
    lhs = jnp.concatenate([cache[s] for s in range(rows)], axis=1)
    sct = nt(lhs, qbd[...]).T
    srope = nn(qrbd, rope[...])
    for s in range(rows):
        part = slice(n_heads * s, n_heads * (s + 1))
        sc = (sct[part] + srope[part]) * scale
        col = lax.broadcasted_iota(jnp.int32, (n_heads, length), 1)
        sc = jnp.where(col < lengths[s], sc, -jnp.inf)
        own = owns[s]
        peak = jnp.maximum(jnp.max(sc, axis=-1, keepdims=True), own)
        pe = jnp.exp(sc - peak)
        oe = jnp.exp(own - peak)
        inv = 1.0 / (jnp.sum(pe, axis=-1, keepdims=True) + oe)
        pw = (pe * inv).astype(BF16)
        ow = (oe * inv).astype(BF16).astype(F32)
        put(pl.ds(n_heads * s, n_heads), nn(pw, cache[s]) + ow * nlr[s])
    for t in range(n_tp):
        cs[t] = get(pl.ds(t, rows, stride=n_heads), latent).astype(BF16)
    to_all(3, "tp", n_tp, me, cs, cr)
    for i in range(10, 16):
        local[i].wait()

    cap = fs.shape[1]
    slots = n_ep * cap
    sl = lax.broadcasted_iota(jnp.int32, (slots, group), 0)
    want = (sl // cap) * n_tp + me
    hit = jnp.zeros((slots, group), F32)
    wgt = jnp.zeros((slots, group), F32)
    for k in range(ids_h.shape[0]):
        m = ids[k : k + 1, :] == want
        hit = jnp.where(m, 1.0, hit)
        wgt = jnp.where(m, rw[k : k + 1, :], wgt)
    before = (
        lax.broadcasted_iota(jnp.int32, (group, group), 0)
        < lax.broadcasted_iota(jnp.int32, (group, group), 1)
    )
    rank = nn(hit.astype(BF16), jnp.where(before, 1.0, 0.0).astype(BF16))
    taken = (hit > 0.5) & (jnp.abs(rank - (sl % cap).astype(F32)) < 0.5)
    disp = jnp.where(taken, 1.0, 0.0).astype(BF16)
    comb = jnp.where(taken, wgt, 0.0)
    comb_hi = comb.astype(BF16)
    comb_lo = (comb - comb_hi.astype(F32)).astype(BF16)

    await_all(3, n_tp, cr)
    for t in range(n_tp):
        put(pl.ds(rows * t, rows), cr[t].astype(F32))
    hv = nt(get(pl.ds(0, group), latent).astype(BF16), wvu[...]).astype(BF16)
    big[...] = nn(hv, wao[...])
    for t in range(n_tp):
        ds_[t % 2, t // 2] = big[pl.ds(rows * t, rows), :].astype(BF16)
    reduce_start(4, ds_, dp)
    for i in range(16, len(jobs)):
        local[i].wait()
    reduce_rest(4, ds_, dp, dm, dr)
    after = tok + reduce_sum(4, dr)
    ee[core, place] = normed_rows(after, fgain[...]).astype(BF16)
    gather(6, ee)
    gather_rest(6, ee)
    for t in range(n_tp):
        big[pl.ds(rows * t, rows), :] = ee[t % 2, t // 2].astype(F32)
    ffn = big[...].astype(BF16)
    out = nn(disp, ffn)
    gate = bg[...].astype(F32)
    dots = big[:, 0:128] * gate[0:1]
    for k in range(1, width // 128):
        dots = dots + big[:, 128 * k : 128 * k + 128] * gate[k : k + 1]
    mix = jax.nn.sigmoid(jnp.sum(dots, axis=-1, keepdims=True))
    small[...] = out
    for g in range(n_ep):
        fs[g] = small[pl.ds(cap * g, cap), :].astype(BF16)
    to_all(8, "ep", n_ep, grp, fs, fr)
    h = nt(ffn, w2[...])
    a, b = sg_h.shape[0], dg_h.shape[0]
    sact = (silu(h[:, 0:a]) * h[:, a : 2 * a]).astype(BF16)
    dact = (silu(h[:, 2 * a : 2 * a + b]) * h[:, 2 * a + b : 2 * a + 2 * b]).astype(BF16)
    await_all(8, n_ep, fr)
    for g in range(n_ep):
        small[pl.ds(cap * g, cap), :] = fr[g].astype(F32)
    arrived = small[...].astype(BF16)
    act = (silu(nn(arrived, eg[...])) * nn(arrived, eu[...])).astype(BF16)
    small[...] = nn(act, ed[...])
    for g in range(n_ep):
        gs[g] = small[pl.ds(cap * g, cap), :].astype(BF16)
    to_all(9, "ep", n_ep, grp, gs, gr)
    big[...] = nn(sact, sd[...]) + mix * nn(dact, dd[...])
    await_all(9, n_ep, gr)
    for g in range(n_ep):
        small[pl.ds(cap * g, cap), :] = gr[g].astype(F32)
    back = small[...].astype(BF16)
    big[...] += tn(comb_hi, back) + tn(comb_lo, back)
    for t in range(n_tp):
        hs[t % 2, t // 2] = big[pl.ds(rows * t, rows), :].astype(BF16)
    reduce_start(10, hs, hp)
    reduce_rest(10, hs, hp, hm, hr)
    for phase, buf in ((0, xa), (6, ee)):
        wait_bytes(send.at[phase], buf.at[0, pl.ds(0, n_z - 1)])
        wait_bytes(send.at[phase + 1], buf.at[0])
    for phase, n, buf in ((2, n_tp, bs), (3, n_tp, cs), (8, n_ep, fs), (9, n_ep, gs)):
        wait_bytes(send.at[phase], buf.at[pl.ds(0, n - 1)])
    for phase, buf in ((4, dp), (10, hp)):
        wait_bytes(send.at[phase], buf)
    wait_bytes(send.at[5], dm.at[pl.ds(0, n_z - 1)])
    total = reduce_sum(10, hr)
    mixed_o[...] = (after + total).astype(BF16)
    wait_bytes(send.at[11], hm.at[pl.ds(0, n_z - 1)])


def local(
    tokens,
    lengths,
    cache_latent,
    cache_rope_key,
    route_ids,
    route_weights,
    attn_gain,
    w_query_nope,
    w_query_rope,
    w_latent_down,
    w_key_rope,
    latent_gain,
    w_key_up,
    w_value_up,
    w_attn_out,
    ffn_gain,
    expert_gate,
    expert_up,
    expert_down,
    shared_gate,
    shared_up,
    shared_down,
    dense_gate,
    dense_up,
    dense_down,
    branch_gate,
):
    n_tp = lax.axis_size("tp")
    n_ep = lax.axis_size("ep")
    rows, width = tokens.shape
    group = rows * n_tp
    wqn = w_query_nope.reshape(width, -1).T
    wqr = w_query_rope.reshape(width, -1).T
    wld = w_latent_down.T
    wkr = w_key_rope.T
    wku = w_key_up.reshape(w_key_up.shape[0], -1).T
    wvu = w_value_up.reshape(w_value_up.shape[0], -1).T
    wao = w_attn_out.reshape(-1, width)
    sg, su, dg, du = shared_gate.T, shared_up.T, dense_gate.T, dense_up.T
    rope = jnp.swapaxes(cache_rope_key, 1, 2).reshape(-1, cache_rope_key.shape[1])
    latent = wku.shape[1]
    ropew = wqr.shape[0]
    cap = max(2, -(-2 * rows * route_ids.shape[1] // n_ep))
    args = [
        lengths,
        tokens,
        cache_latent,
        rope,
        route_ids.T,
        route_weights.T,
        attn_gain.reshape(1, -1),
        wqn,
        wqr,
        wld,
        wkr,
        latent_gain.reshape(1, -1),
        wku,
        wvu,
        wao,
        ffn_gain.reshape(1, -1),
        expert_gate[0],
        expert_up[0],
        expert_down[0],
        sg,
        su,
        shared_down,
        dg,
        du,
        dense_down,
        branch_gate.reshape(-1, 128),
    ]
    any_spec = pl.BlockSpec(memory_space=pl.ANY)
    vm = lambda a: pltpu.VMEM(a.shape, a.dtype)
    n1 = wqn.shape[0] + ropew + wld.shape[0]
    n2 = 2 * (sg.shape[0] + dg.shape[0])
    wide = latent + 128
    scratch = [
        vm(cache_latent),
        vm(rope),
        vm(args[4]),
        vm(args[5]),
        vm(args[6]),
        pltpu.VMEM((n1, width), BF16),
        vm(wkr),
        vm(args[11]),
        vm(wku),
        vm(wvu),
        vm(wao),
        vm(args[15]),
        vm(args[16]),
        vm(args[17]),
        vm(args[18]),
        pltpu.VMEM((n2, width), BF16),
        vm(shared_down),
        vm(dense_down),
        vm(args[25]),
        pltpu.VMEM((2, n_tp // 2, rows, width), BF16),
        pltpu.VMEM((n_tp, rows, wide), BF16),
        pltpu.VMEM((n_tp, rows, wide), BF16),
        pltpu.VMEM((n_tp, rows, latent), BF16),
        pltpu.VMEM((n_tp, rows, latent), BF16),
        pltpu.VMEM((2, n_tp // 2, rows, width), BF16),
        pltpu.VMEM((n_tp // 2, rows, width), BF16),
        pltpu.VMEM((n_tp // 2, rows, width), BF16),
        pltpu.VMEM((n_tp // 2, rows, width), BF16),
        pltpu.VMEM((2, n_tp // 2, rows, width), BF16),
        pltpu.VMEM((n_ep, cap, width), BF16),
        pltpu.VMEM((n_ep, cap, width), BF16),
        pltpu.VMEM((n_ep, cap, width), BF16),
        pltpu.VMEM((n_ep, cap, width), BF16),
        pltpu.VMEM((2, n_tp // 2, rows, width), BF16),
        pltpu.VMEM((n_tp // 2, rows, width), BF16),
        pltpu.VMEM((n_tp // 2, rows, width), BF16),
        pltpu.VMEM((n_tp // 2, rows, width), BF16),
        pltpu.VMEM((-(-group // 128) * 128, rows * latent), BF16),
        pltpu.VMEM((group, width), F32),
        pltpu.VMEM((n_ep * cap, width), F32),
        pltpu.VMEM((wide // 128, group, 128), F32),
        pltpu.VMEM((rows, 128), F32),
        pltpu.SemaphoreType.DMA((25,)),
        pltpu.SemaphoreType.DMA((12,)),
        pltpu.SemaphoreType.DMA((12,)),
    ]
    found = pl.pallas_call(
        functools.partial(layer_kernel, n_tp, n_ep),
        out_shape=(
            jax.ShapeDtypeStruct((rows, width), BF16),
            jax.ShapeDtypeStruct((rows, latent), BF16),
            jax.ShapeDtypeStruct((rows, ropew), BF16),
        ),
        in_specs=[pl.BlockSpec(memory_space=pltpu.SMEM)] + [any_spec] * 25,
        out_specs=(pl.BlockSpec(memory_space=pltpu.VMEM),) * 3,
        scratch_shapes=scratch,
        compiler_params=pltpu.CompilerParams(
            collective_id=0, has_side_effects=True, vmem_limit_bytes=56 * 1024 * 1024
        ),
        name="layer",
    )(*args)
    vmem = pl.BlockSpec(memory_space=pltpu.VMEM)
    return pl.pallas_call(
        finish_kernel,
        out_shape=tuple(jax.ShapeDtypeStruct(a.shape, a.dtype) for a in found),
        in_specs=[vmem] * 3,
        out_specs=(vmem,) * 3,
        name="finish",
    )(*found)


def solution(mesh):
    in_specs = (
        P(("ep", "tp"), None),
        P(("ep", "tp")),
        P(("ep", "tp"), None, None),
        P(("ep", "tp"), None, None),
        P("ep", None),
        P("ep", None),
        P(),
        P(None, "tp", None),
        P(None, "tp", None),
        P(None, "tp"),
        P(),
        P(),
        P(None, "tp", None),
        P(None, "tp", None),
        P("tp", None, None),
        P(),
        P(("ep", "tp"), None, None),
        P(("ep", "tp"), None, None),
        P(("ep", "tp"), None, None),
        P(None, "tp"),
        P(None, "tp"),
        P("tp", None),
        P(None, "tp"),
        P(None, "tp"),
        P("tp", None),
        P(),
    )
    out_specs = (P(("ep", "tp"), None), P(("ep", "tp"), None), P(("ep", "tp"), None))
    return jax.shard_map(local, mesh=mesh, in_specs=in_specs, out_specs=out_specs, check_vma=False)
```

```python
import functools

import jax
import jax.numpy as jnp
from jax import lax
from jax.experimental import pallas as pl
from jax.experimental.pallas import tpu as pltpu
from jax.sharding import PartitionSpec as P

EPS = 1e-06
ROPE_BASE = 10000.0
MESH = pl.DeviceIdType.MESH
F32 = jnp.float32
BF16 = jnp.bfloat16


def nn(a, b):
    return lax.dot_general(a, b, (((1,), (0,)), ((), ())), preferred_element_type=F32)


def nt(a, b):
    return lax.dot_general(a, b, (((1,), (1,)), ((), ())), preferred_element_type=F32)


def tn(a, b):
    return lax.dot_general(a, b, (((0,), (0,)), ((), ())), preferred_element_type=F32)


def normed_rows(x, gain):
    return x * lax.rsqrt(jnp.mean(x * x, axis=-1, keepdims=True) + EPS) * gain


def silu(v):
    return v / (1.0 + jnp.exp(-v))


def finish_kernel(mixed, nlat, nrope, mixed_o, nlat_o, nrope_o):
    mixed_o[...] = mixed[...]
    nlat_o[...] = nlat[...]
    nrope_o[...] = nrope[...]


def layer_kernel(
    n_tp,
    n_ep,
    lengths_h,
    tokens,
    cache_h,
    rope_h,
    ids_h,
    rw_h,
    again_h,
    wqn_h,
    wqr_h,
    wld_h,
    wkr_h,
    lgain_h,
    wku_h,
    wvu_h,
    wao_h,
    fgain_h,
    eg_h,
    eu_h,
    ed_h,
    sg_h,
    su_h,
    sd_h,
    dg_h,
    du_h,
    dd_h,
    bg_h,
    mixed_o,
    nlat_o,
    nrope_o,
    lengths,
    cache,
    rope,
    ids,
    rw,
    again,
    w1,
    wkr,
    lgain,
    wku,
    wvu,
    wao,
    fgain,
    eg,
    eu,
    ed,
    w2,
    sd,
    dd,
    bg,
    xa,
    bs,
    br,
    cs,
    cr,
    ds_,
    dp,
    dm,
    dr,
    ee,
    fs,
    fr,
    gs,
    gr,
    hs,
    hp,
    hm,
    hr,
    sco,
    prob,
    big,
    small,
    rf,
    krs,
    lsem,
    send,
    recv,
):
    me = lax.axis_index("tp")
    grp = lax.axis_index("ep")
    rows, width = tokens.shape
    group = rows * n_tp
    nope = wqn_h.shape[0]
    ropew = wqr_h.shape[0]
    latw = wld_h.shape[0]
    latent = wku_h.shape[1]
    length = cache.shape[1]
    scale = (nope + ropew) ** (-0.5)

    wide = latent + 128
    n_z = n_tp // 2
    core = lax.rem(me, 2)
    place = lax.div(me, 2)

    def put(where, value):
        for k in range(value.shape[1] // 128):
            rf[k, where, :] = value[:, 128 * k : 128 * k + 128]

    def get(where, columns):
        return jnp.concatenate([rf[k, where, :] for k in range(columns // 128)], axis=1)

    jobs = [
        (tokens, xa.at[core, place]),
        (again_h, again),
        (wqn_h, w1.at[pl.ds(0, nope)]),
        (wqr_h, w1.at[pl.ds(nope, ropew)]),
        (wld_h, w1.at[pl.ds(nope + ropew, latw)]),
        (wkr_h, wkr),
        (wku_h, wku),
        (lgain_h, lgain),
        (cache_h, cache),
        (rope_h, rope),
        (wvu_h, wvu),
        (wao_h, wao),
        (fgain_h, fgain),
        (ids_h, ids),
        (rw_h, rw),
        (bg_h, bg),
        (sg_h, w2.at[pl.ds(0, sg_h.shape[0])]),
        (su_h, w2.at[pl.ds(sg_h.shape[0], sg_h.shape[0])]),
        (dg_h, w2.at[pl.ds(2 * sg_h.shape[0], dg_h.shape[0])]),
        (du_h, w2.at[pl.ds(2 * sg_h.shape[0] + dg_h.shape[0], dg_h.shape[0])]),
        (eg_h, eg),
        (eu_h, eu),
        (ed_h, ed),
        (sd_h, sd),
        (dd_h, dd),
        (lengths_h, lengths),
    ]
    local = [pltpu.make_async_copy(s, d, lsem.at[i]) for i, (s, d) in enumerate(jobs)]
    for c in local:
        c.start()

    barrier = pltpu.get_barrier_semaphore()

    def greet(i, _):
        pl.semaphore_signal(
            barrier, inc=1, device_id={"tp": lax.rem(me + i, n_tp)}, device_id_type=MESH
        )
        return 0

    def greet_ep(i, _):
        pl.semaphore_signal(
            barrier, inc=1, device_id={"ep": lax.rem(grp + i, n_ep)}, device_id_type=MESH
        )
        return 0

    lax.fori_loop(1, n_tp, greet, 0)
    lax.fori_loop(1, n_ep, greet_ep, 0)

    def hop(phase, axis, to, src, dst):
        return pltpu.make_async_remote_copy(
            src_ref=src,
            dst_ref=dst,
            send_sem=send.at[phase],
            recv_sem=recv.at[phase],
            device_id={axis: to},
            device_id_type=MESH,
        )

    def wait_bytes(sem, like):
        pltpu.make_async_copy(like, like, sem).wait()

    def near(n):
        return sorted(range(n), key=lambda d: (-min(d, n - d), d))

    def to_all_tp(phase, src, dst):
        for d in near(n_z):
            for k in range(2):
                if d or k:
                    to = 2 * lax.rem(place + d, n_z) + lax.rem(core + k, 2)
                    hop(phase, "tp", to, src.at[to], dst.at[me]).start()
        dst[me] = src[me]

    side = int(n_ep**0.5)
    side = side if side * side == n_ep else 1
    across = n_ep // side

    def to_all_ep(phase, src, dst):
        y, x = lax.div(grp, across), lax.rem(grp, across)
        offsets = [(dy, dx) for dy in range(side) for dx in range(across) if dy or dx]
        offsets.sort(key=lambda o: -min(o[0], side - o[0]) - min(o[1], across - o[1]))
        for dy, dx in offsets:
            to = lax.rem(y + dy, side) * across + lax.rem(x + dx, across)
            hop(phase, "ep", to, src.at[to], dst.at[grp]).start()
        dst[grp] = src[grp]

    def await_all(phase, n, dst):
        wait_bytes(recv.at[phase], dst.at[pl.ds(0, n - 1)])

    def along_z(phase, pick, dst):
        for d in near(n_z):
            if d:
                z = lax.rem(place + d, n_z)
                hop(phase, "tp", 2 * z + core, pick(z), dst).start()

    def gather(phase, buf):
        along_z(phase, lambda to: buf.at[core, place], buf.at[core, place])

    def gather_rest(phase, buf):
        wait_bytes(recv.at[phase], buf.at[0, pl.ds(0, n_z - 1)])
        hop(phase + 1, "tp", 2 * place + 1 - core, buf.at[core], buf.at[core]).start()
        wait_bytes(recv.at[phase + 1], buf.at[0])

    def reduce_start(phase, src, pair):
        hop(phase, "tp", 2 * place + 1 - core, src.at[1 - core], pair).start()

    def reduce_rest(phase, src, pair, mid, dst):
        wait_bytes(recv.at[phase], pair)
        for z in range(n_z):
            mid[z] = (src[core, z].astype(F32) + pair[z].astype(F32)).astype(BF16)
        along_z(phase + 1, lambda to: mid.at[to], dst.at[place])
        dst[place] = mid[place]

    def reduce_sum(phase, dst):
        wait_bytes(recv.at[phase + 1], dst.at[pl.ds(0, n_z - 1)])
        total = dst[0].astype(F32)
        for z in range(1, n_z):
            total = total + dst[z].astype(F32)
        return total

    local[25].wait()
    lane = lax.broadcasted_iota(jnp.int32, (rows, 128), 1)
    rowi = lax.broadcasted_iota(jnp.int32, (rows, 128), 0)
    half = ropew // 2
    freq = jnp.zeros((rows, 128), F32)
    for i in range(half):
        freq = jnp.where(lane % half == i, F32(ROPE_BASE ** (-i / half)), freq)
    pos = jnp.zeros((rows, 128), jnp.int32)
    for s in range(rows):
        pos = jnp.where(rowi == s, lengths[s], pos)
    angle = pos.astype(F32) * freq
    cosv = jnp.cos(angle)
    sinv = jnp.sin(angle)

    def rotated(v, c, s):
        ln = lax.broadcasted_iota(jnp.int32, v.shape, 1)
        other = jnp.where(
            ln % ropew < half, -pltpu.roll(v, 128 - half, 1), pltpu.roll(v, half, 1)
        )
        return v * c + other * s

    pl.semaphore_wait(barrier, (n_tp - 1) + (n_ep - 1))
    local[0].wait()
    gather(0, xa)

    local[1].wait()
    local[5].wait()
    tok = xa[core, place].astype(F32)
    own_normed = normed_rows(tok, again[...]).astype(BF16)
    krs[...] = jnp.zeros_like(krs)
    krs[:, 0:ropew] = nt(own_normed, wkr[...])
    new_rope = rotated(krs[...], cosv, sinv).astype(BF16).astype(F32)
    nrope_o[...] = new_rope[:, 0:ropew].astype(BF16)
    for i in (2, 3, 4, 6, 7):
        local[i].wait()

    gather_rest(0, xa)
    for t in range(n_tp):
        big[pl.ds(rows * t, rows), :] = xa[t % 2, t // 2].astype(F32)
    normed = normed_rows(big[...], again[...]).astype(BF16)
    y = nt(normed, w1[...])
    ql = nn(y[:, 0:nope].astype(BF16), wku[...])
    put(pl.ds(0, group), jnp.concatenate([ql, y], axis=1))
    for t in range(n_tp):
        bs[t] = get(pl.ds(rows * t, rows), wide).astype(BF16)
    to_all_tp(2, bs, br)
    await_all(2, n_tp, br)
    for t in range(n_tp):
        put(pl.ds(rows * t, rows), br[t].astype(F32))

    parts = []
    ln4 = lax.broadcasted_iota(jnp.int32, (rows, 128), 1)
    per = 128 // latw
    for k in range(latent // 128):
        acc = jnp.zeros((rows, 128), F32)
        for j in range(per):
            piece = br[k * per + j][:, latent : latent + 128].astype(F32)
            shift = (j * latw - (nope + ropew)) % 128
            if shift:
                piece = pltpu.roll(piece, shift, 1)
            acc = jnp.where(ln4 // latw == j, piece, acc)
        parts.append(acc)
    latent_raw = jnp.concatenate(parts, axis=1)
    nl16 = normed_rows(latent_raw, lgain[...]).astype(BF16)
    nlat_o[...] = nl16
    new_latent = nl16.astype(F32)
    lane_r = lax.broadcasted_iota(jnp.int32, (rows, 128), 1)
    nr_al = jnp.where(
        (lane_r >= nope) & (lane_r < nope + ropew), pltpu.roll(new_rope, nope, 1), 0.0
    )

    local[8].wait()
    local[9].wait()
    n_heads = n_tp
    nlr = [new_latent[s : s + 1] for s in range(rows)]
    qrots, owns = [], []
    for s in range(rows):
        q = get(pl.ds(s, n_heads, stride=rows), latent)
        qr = rf[latent // 128, pl.ds(s, n_heads, stride=rows), :]
        sco[s] = nt(q.astype(BF16), cache[s])
        qrot = rotated(qr, cosv[s : s + 1], sinv[s : s + 1]).astype(BF16).astype(F32)
        owns.append(
            (
                jnp.sum(q * nlr[s], axis=-1, keepdims=True)
                + jnp.sum(qrot * nr_al[s : s + 1], axis=-1, keepdims=True)
            )
            * scale
        )
        shift = (ropew * s - nope) % 128
        lnq = lax.broadcasted_iota(jnp.int32, qrot.shape, 1)
        qrots.append(
            jnp.where(lnq // ropew == s, pltpu.roll(qrot, shift, 1) if shift else qrot, 0.0)
        )
    qrbd = jnp.concatenate(qrots, axis=0).astype(BF16)
    srope = nn(qrbd, rope[...])
    own_w = []
    for s in range(rows):
        sc = (sco[s] + srope[n_heads * s : n_heads * (s + 1)]) * scale
        col = lax.broadcasted_iota(jnp.int32, (n_heads, length), 1)
        sc = jnp.where(col < lengths[s], sc, -jnp.inf)
        own = owns[s]
        peak = jnp.maximum(jnp.max(sc, axis=-1, keepdims=True), own)
        pe = jnp.exp(sc - peak)
        oe = jnp.exp(own - peak)
        inv = 1.0 / (jnp.sum(pe, axis=-1, keepdims=True) + oe)
        prob[s] = (pe * inv).astype(BF16)
        own_w.append((oe * inv).astype(BF16).astype(F32))
    for s in range(rows):
        out = nn(prob[s], cache[s]) + own_w[s] * nlr[s]
        put(pl.ds(n_heads * s, n_heads), out)
    for t in range(n_tp):
        cs[t] = get(pl.ds(t, rows, stride=n_heads), latent).astype(BF16)
    to_all_tp(3, cs, cr)
    for i in range(10, 16):
        local[i].wait()

    cap = fs.shape[1]
    slots = n_ep * cap
    sl = lax.broadcasted_iota(jnp.int32, (slots, group), 0)
    want = (sl // cap) * n_tp + me
    hit = jnp.zeros((slots, group), F32)
    wgt = jnp.zeros((slots, group), F32)
    for k in range(ids_h.shape[0]):
        m = ids[k : k + 1, :] == want
        hit = jnp.where(m, 1.0, hit)
        wgt = jnp.where(m, rw[k : k + 1, :], wgt)
    before = (
        lax.broadcasted_iota(jnp.int32, (group, group), 0)
        < lax.broadcasted_iota(jnp.int32, (group, group), 1)
    )
    rank = nn(hit.astype(BF16), jnp.where(before, 1.0, 0.0).astype(BF16))
    taken = (hit > 0.5) & (jnp.abs(rank - (sl % cap).astype(F32)) < 0.5)
    disp = jnp.where(taken, 1.0, 0.0).astype(BF16)
    comb = jnp.where(taken, wgt, 0.0)
    comb_hi = comb.astype(BF16)
    comb_lo = (comb - comb_hi.astype(F32)).astype(BF16)

    await_all(3, n_tp, cr)
    for t in range(n_tp):
        put(pl.ds(rows * t, rows), cr[t].astype(F32))
    hv = nt(get(pl.ds(0, group), latent).astype(BF16), wvu[...]).astype(BF16)
    big[...] = nn(hv, wao[...])
    for t in range(n_tp):
        ds_[t % 2, t // 2] = big[pl.ds(rows * t, rows), :].astype(BF16)
    reduce_start(4, ds_, dp)
    for i in range(16, 25):
        local[i].wait()
    reduce_rest(4, ds_, dp, dm, dr)
    after = tok + reduce_sum(4, dr)
    ee[core, place] = normed_rows(after, fgain[...]).astype(BF16)
    gather(6, ee)
    gather_rest(6, ee)
    for t in range(n_tp):
        big[pl.ds(rows * t, rows), :] = ee[t % 2, t // 2].astype(F32)
    ffn = big[...].astype(BF16)
    out = nn(disp, ffn)
    gate = bg[...].astype(F32)
    dots = big[:, 0:128] * gate[0:1]
    for k in range(1, width // 128):
        dots = dots + big[:, 128 * k : 128 * k + 128] * gate[k : k + 1]
    mix = jax.nn.sigmoid(jnp.sum(dots, axis=-1, keepdims=True))
    small[...] = out
    for g in range(n_ep):
        fs[g] = small[pl.ds(cap * g, cap), :].astype(BF16)
    to_all_ep(8, fs, fr)
    h = nt(ffn, w2[...])
    a, b = sg_h.shape[0], dg_h.shape[0]
    sact = (silu(h[:, 0:a]) * h[:, a : 2 * a]).astype(BF16)
    dact = (silu(h[:, 2 * a : 2 * a + b]) * h[:, 2 * a + b : 2 * a + 2 * b]).astype(BF16)
    await_all(8, n_ep, fr)
    for g in range(n_ep):
        small[pl.ds(cap * g, cap), :] = fr[g].astype(F32)
    arrived = small[...].astype(BF16)
    act = (silu(nn(arrived, eg[...])) * nn(arrived, eu[...])).astype(BF16)
    small[...] = nn(act, ed[...])
    for g in range(n_ep):
        gs[g] = small[pl.ds(cap * g, cap), :].astype(BF16)
    to_all_ep(9, gs, gr)
    big[...] = nn(sact, sd[...]) + mix * nn(dact, dd[...])
    await_all(9, n_ep, gr)
    for g in range(n_ep):
        small[pl.ds(cap * g, cap), :] = gr[g].astype(F32)
    back = small[...].astype(BF16)
    big[...] += tn(comb_hi, back) + tn(comb_lo, back)
    for t in range(n_tp):
        hs[t % 2, t // 2] = big[pl.ds(rows * t, rows), :].astype(BF16)
    reduce_start(10, hs, hp)
    reduce_rest(10, hs, hp, hm, hr)
    for phase, buf in ((0, xa), (6, ee)):
        wait_bytes(send.at[phase], buf.at[0, pl.ds(0, n_z - 1)])
        wait_bytes(send.at[phase + 1], buf.at[0])
    for phase, n, buf in ((2, n_tp, bs), (3, n_tp, cs), (8, n_ep, fs), (9, n_ep, gs)):
        wait_bytes(send.at[phase], buf.at[pl.ds(0, n - 1)])
    for phase, buf in ((4, dp), (10, hp)):
        wait_bytes(send.at[phase], buf)
    wait_bytes(send.at[5], dm.at[pl.ds(0, n_z - 1)])
    total = reduce_sum(10, hr)
    mixed_o[...] = (after + total).astype(BF16)
    wait_bytes(send.at[11], hm.at[pl.ds(0, n_z - 1)])


def local(
    tokens,
    lengths,
    cache_latent,
    cache_rope_key,
    route_ids,
    route_weights,
    attn_gain,
    w_query_nope,
    w_query_rope,
    w_latent_down,
    w_key_rope,
    latent_gain,
    w_key_up,
    w_value_up,
    w_attn_out,
    ffn_gain,
    expert_gate,
    expert_up,
    expert_down,
    shared_gate,
    shared_up,
    shared_down,
    dense_gate,
    dense_up,
    dense_down,
    branch_gate,
):
    n_tp = lax.axis_size("tp")
    n_ep = lax.axis_size("ep")
    rows, width = tokens.shape
    group = rows * n_tp
    wqn = w_query_nope.reshape(width, -1).T
    wqr = w_query_rope.reshape(width, -1).T
    wld = w_latent_down.T
    wkr = w_key_rope.T
    wku = w_key_up.reshape(w_key_up.shape[0], -1).T
    wvu = w_value_up.reshape(w_value_up.shape[0], -1).T
    wao = w_attn_out.reshape(-1, width)
    sg, su, dg, du = shared_gate.T, shared_up.T, dense_gate.T, dense_up.T
    rope = jnp.swapaxes(cache_rope_key, 1, 2).reshape(-1, cache_rope_key.shape[1])
    latent = wku.shape[1]
    ropew = wqr.shape[0]
    cap = max(2, -(-2 * rows * route_ids.shape[1] // n_ep))
    args = [
        lengths,
        tokens,
        cache_latent,
        rope,
        route_ids.T,
        route_weights.T,
        attn_gain.reshape(1, -1),
        wqn,
        wqr,
        wld,
        wkr,
        latent_gain.reshape(1, -1),
        wku,
        wvu,
        wao,
        ffn_gain.reshape(1, -1),
        expert_gate[0],
        expert_up[0],
        expert_down[0],
        sg,
        su,
        shared_down,
        dg,
        du,
        dense_down,
        branch_gate.reshape(-1, 128),
    ]
    hbm_spec = pl.BlockSpec(memory_space=pltpu.HBM)
    vm = lambda a: pltpu.VMEM(a.shape, a.dtype)
    n1 = wqn.shape[0] + ropew + wld.shape[0]
    n2 = 2 * (sg.shape[0] + dg.shape[0])
    wide = latent + 128
    scratch = [
        pltpu.SMEM(lengths.shape, jnp.int32),
        vm(cache_latent),
        vm(rope),
        vm(args[4]),
        vm(args[5]),
        vm(args[6]),
        pltpu.VMEM((n1, width), BF16),
        vm(wkr),
        vm(args[11]),
        vm(wku),
        vm(wvu),
        vm(wao),
        vm(args[15]),
        vm(args[16]),
        vm(args[17]),
        vm(args[18]),
        pltpu.VMEM((n2, width), BF16),
        vm(shared_down),
        vm(dense_down),
        vm(args[25]),
        pltpu.VMEM((2, n_tp // 2, rows, width), BF16),
        pltpu.VMEM((n_tp, rows, wide), BF16),
        pltpu.VMEM((n_tp, rows, wide), BF16),
        pltpu.VMEM((n_tp, rows, latent), BF16),
        pltpu.VMEM((n_tp, rows, latent), BF16),
        pltpu.VMEM((2, n_tp // 2, rows, width), BF16),
        pltpu.VMEM((n_tp // 2, rows, width), BF16),
        pltpu.VMEM((n_tp // 2, rows, width), BF16),
        pltpu.VMEM((n_tp // 2, rows, width), BF16),
        pltpu.VMEM((2, n_tp // 2, rows, width), BF16),
        pltpu.VMEM((n_ep, cap, width), BF16),
        pltpu.VMEM((n_ep, cap, width), BF16),
        pltpu.VMEM((n_ep, cap, width), BF16),
        pltpu.VMEM((n_ep, cap, width), BF16),
        pltpu.VMEM((2, n_tp // 2, rows, width), BF16),
        pltpu.VMEM((n_tp // 2, rows, width), BF16),
        pltpu.VMEM((n_tp // 2, rows, width), BF16),
        pltpu.VMEM((n_tp // 2, rows, width), BF16),
        pltpu.VMEM((rows, n_tp, cache_latent.shape[1]), F32),
        pltpu.VMEM((rows, n_tp, cache_latent.shape[1]), BF16),
        pltpu.VMEM((group, width), F32),
        pltpu.VMEM((n_ep * cap, width), F32),
        pltpu.VMEM((wide // 128, group, 128), F32),
        pltpu.VMEM((rows, 128), F32),
        pltpu.SemaphoreType.DMA((26,)),
        pltpu.SemaphoreType.DMA((12,)),
        pltpu.SemaphoreType.DMA((12,)),
    ]
    found = pl.pallas_call(
        functools.partial(layer_kernel, n_tp, n_ep),
        out_shape=(
            jax.ShapeDtypeStruct((rows, width), BF16),
            jax.ShapeDtypeStruct((rows, latent), BF16),
            jax.ShapeDtypeStruct((rows, ropew), BF16),
        ),
        in_specs=[hbm_spec] * 26,
        out_specs=(pl.BlockSpec(memory_space=pltpu.VMEM),) * 3,
        scratch_shapes=scratch,
        compiler_params=pltpu.CompilerParams(
            collective_id=0, has_side_effects=True, vmem_limit_bytes=40 * 1024 * 1024
        ),
        name="layer",
    )(*[pltpu.with_memory_space_constraint(a, pltpu.HBM) for a in args])
    vmem = pl.BlockSpec(memory_space=pltpu.VMEM)
    return pl.pallas_call(
        finish_kernel,
        out_shape=tuple(jax.ShapeDtypeStruct(a.shape, a.dtype) for a in found),
        in_specs=[vmem] * 3,
        out_specs=(vmem,) * 3,
        compiler_params=pltpu.CompilerParams(vmem_limit_bytes=8 * 1024 * 1024),
        name="finish",
    )(*found)


def solution(mesh):
    in_specs = (
        P(("ep", "tp"), None),
        P(("ep", "tp")),
        P(("ep", "tp"), None, None),
        P(("ep", "tp"), None, None),
        P("ep", None),
        P("ep", None),
        P(),
        P(None, "tp", None),
        P(None, "tp", None),
        P(None, "tp"),
        P(),
        P(),
        P(None, "tp", None),
        P(None, "tp", None),
        P("tp", None, None),
        P(),
        P(("ep", "tp"), None, None),
        P(("ep", "tp"), None, None),
        P(("ep", "tp"), None, None),
        P(None, "tp"),
        P(None, "tp"),
        P("tp", None),
        P(None, "tp"),
        P(None, "tp"),
        P("tp", None),
        P(),
    )
    out_specs = (P(("ep", "tp"), None), P(("ep", "tp"), None), P(("ep", "tp"), None))
    return jax.shard_map(local, mesh=mesh, in_specs=in_specs, out_specs=out_specs, check_vma=False)
```

```python
import functools

import jax
import jax.numpy as jnp
from jax import lax
from jax.experimental import pallas as pl
from jax.experimental.pallas import tpu as pltpu
from jax.sharding import PartitionSpec as P

EPS = 1e-06
ROPE_BASE = 10000.0
MESH = pl.DeviceIdType.MESH
F32 = jnp.float32
BF16 = jnp.bfloat16


def nn(a, b):
    return lax.dot_general(a, b, (((1,), (0,)), ((), ())), preferred_element_type=F32)


def nt(a, b):
    return lax.dot_general(a, b, (((1,), (1,)), ((), ())), preferred_element_type=F32)


def tn(a, b):
    return lax.dot_general(a, b, (((0,), (0,)), ((), ())), preferred_element_type=F32)


def normed_rows(x, gain):
    return x * lax.rsqrt(jnp.mean(x * x, axis=-1, keepdims=True) + EPS) * gain


def silu(v):
    return v / (1.0 + jnp.exp(-v))


def finish_kernel(mixed, nlat, nrope, mixed_o, nlat_o, nrope_o):
    mixed_o[...] = mixed[...]
    nlat_o[...] = nlat[...]
    nrope_o[...] = nrope[...]


def layer_kernel(
    n_tp,
    n_ep,
    lengths_h,
    tokens,
    cache_h,
    rope_h,
    ids_h,
    rw_h,
    again_h,
    wqn_h,
    wqr_h,
    wld_h,
    wkr_h,
    lgain_h,
    wku_h,
    wvu_h,
    wao_h,
    fgain_h,
    eg_h,
    eu_h,
    ed_h,
    sg_h,
    su_h,
    sd_h,
    dg_h,
    du_h,
    dd_h,
    bg_h,
    mixed_o,
    nlat_o,
    nrope_o,
    lengths,
    cache,
    rope,
    ids,
    rw,
    again,
    w1,
    wkr,
    lgain,
    wku,
    wvu,
    wao,
    fgain,
    eg,
    eu,
    ed,
    w2,
    sd,
    dd,
    bg,
    xo,
    xa,
    bs,
    br,
    cs,
    cr,
    ds_,
    dr,
    ee,
    fs,
    fr,
    gs,
    gr,
    hs,
    hp,
    hm,
    hr,
    sco,
    prob,
    big,
    small,
    rf,
    krs,
    lsem,
    send,
    recv,
    each,
):
    me = lax.axis_index("tp")
    grp = lax.axis_index("ep")
    rows, width = tokens.shape
    group = rows * n_tp
    nope = wqn_h.shape[0]
    ropew = wqr_h.shape[0]
    latw = wld_h.shape[0]
    latent = wku_h.shape[1]
    length = cache.shape[1]
    scale = (nope + ropew) ** (-0.5)

    wide = latent + 128
    n_z = n_tp // 2
    core = lax.rem(me, 2)
    place = lax.div(me, 2)
    other = 2 * place + 1 - core

    def put(where, value):
        for k in range(value.shape[1] // 128):
            rf[k, where, :] = value[:, 128 * k : 128 * k + 128]

    def get(where, columns):
        return jnp.concatenate([rf[k, where, :] for k in range(columns // 128)], axis=1)

    jobs = [
        (tokens, xo),
        (again_h, again),
        (wqn_h, w1.at[core, pl.ds(0, nope)]),
        (wqr_h, w1.at[core, pl.ds(nope, ropew)]),
        (wld_h, w1.at[core, pl.ds(nope + ropew, latw)]),
        (wkr_h, wkr),
        (wku_h, wku.at[core]),
        (lgain_h, lgain),
        (cache_h, cache),
        (rope_h, rope),
        (wvu_h, wvu.at[core]),
        (wao_h, wao.at[core]),
        (fgain_h, fgain),
        (ids_h, ids),
        (rw_h, rw),
        (bg_h, bg),
        (sg_h, w2.at[pl.ds(0, sg_h.shape[0])]),
        (su_h, w2.at[pl.ds(sg_h.shape[0], sg_h.shape[0])]),
        (dg_h, w2.at[pl.ds(2 * sg_h.shape[0], dg_h.shape[0])]),
        (du_h, w2.at[pl.ds(2 * sg_h.shape[0] + dg_h.shape[0], dg_h.shape[0])]),
        (eg_h, eg),
        (eu_h, eu),
        (ed_h, ed),
        (sd_h, sd),
        (dd_h, dd),
        (lengths_h, lengths),
    ]
    local = [pltpu.make_async_copy(s, d, lsem.at[i]) for i, (s, d) in enumerate(jobs)]
    barrier = pltpu.get_barrier_semaphore()

    def near(n):
        return sorted(range(n), key=lambda d: (-min(d, n - d), d))

    for d in near(n_z):
        for k in range(2):
            if d or k:
                to = 2 * lax.rem(place + d, n_z) + lax.rem(core + k, 2)
                pl.semaphore_signal(barrier, inc=1, device_id={"tp": to}, device_id_type=MESH)
    for d in near(n_ep):
        if d:
            to = lax.rem(grp + d, n_ep)
            pl.semaphore_signal(barrier, inc=1, device_id={"ep": to}, device_id_type=MESH)
    for c in local:
        c.start()

    def hop(phase, axis, to, src, dst, got=None):
        return pltpu.make_async_remote_copy(
            src_ref=src,
            dst_ref=dst,
            send_sem=send.at[phase],
            recv_sem=recv.at[phase] if got is None else got,
            device_id={axis: to},
            device_id_type=MESH,
        )

    def wait_bytes(sem, like):
        pltpu.make_async_copy(like, like, sem).wait()

    def to_line(phase, src, dst):
        for d in near(n_z):
            z = lax.rem(place + d, n_z)
            hop(phase, "tp", 2 * z + 1 - core, src.at[z], dst.at[place]).start()

    def await_line(phase, dst):
        wait_bytes(recv.at[phase], dst)

    side = int(n_ep**0.5)
    side = side if side * side == n_ep else 1
    across = n_ep // side

    def to_all_ep(phase, src, dst):
        y, x = lax.div(grp, across), lax.rem(grp, across)
        offsets = [(dy, dx) for dy in range(side) for dx in range(across) if dy or dx]
        offsets.sort(key=lambda o: -min(o[0], side - o[0]) - min(o[1], across - o[1]))
        for dy, dx in offsets:
            to = lax.rem(y + dy, side) * across + lax.rem(x + dx, across)
            hop(phase, "ep", to, src.at[to], dst.at[grp]).start()
        dst[grp] = src[grp]

    def await_all(phase, n, dst):
        wait_bytes(recv.at[phase], dst.at[pl.ds(0, n - 1)])


    def gather(phase, row, buf):
        own = buf.at[core, place]
        for d in near(n_z):
            if d:
                z = lax.rem(place + d, n_z)
                hop(phase, "tp", 2 * z + core, own, own, each.at[row, d]).start()
        hop(phase + 1, "tp", other, own, own).start()

    def gather_rest(phase, row, buf):
        for d in near(n_z):
            if d:
                block = buf.at[core, lax.rem(place + n_z - d, n_z)]
                wait_bytes(each.at[row, d], block)
                hop(phase + 1, "tp", other, block, block).start()
        wait_bytes(recv.at[phase + 1], buf.at[0])

    def reduce_start(phase, row, src, pair):
        for d in near(n_z):
            z = lax.rem(place + d, n_z)
            hop(phase, "tp", other, src.at[1 - core, z], pair.at[z], each.at[row, d]).start()

    def reduce_rest(phase, row, src, pair, mid, dst):
        for d in near(n_z):
            z = lax.rem(place + d, n_z)
            wait_bytes(each.at[row, d], pair.at[z])
            mid[z] = (src[core, z].astype(F32) + pair[z].astype(F32)).astype(BF16)
            if d:
                hop(phase + 1, "tp", 2 * z + core, mid.at[z], dst.at[place]).start()
            else:
                dst[place] = mid[z]

    def reduce_sum(phase, dst):
        wait_bytes(recv.at[phase + 1], dst.at[pl.ds(0, n_z - 1)])
        return line_sum(dst)

    def line_sum(dst):
        total = dst[0].astype(F32)
        for z in range(1, n_z):
            total = total + dst[z].astype(F32)
        return total

    local[25].wait()
    lane = lax.broadcasted_iota(jnp.int32, (rows, 128), 1)
    rowi = lax.broadcasted_iota(jnp.int32, (rows, 128), 0)
    half = ropew // 2
    freq = jnp.zeros((rows, 128), F32)
    for i in range(half):
        freq = jnp.where(lane % half == i, F32(ROPE_BASE ** (-i / half)), freq)
    pos = jnp.zeros((rows, 128), jnp.int32)
    for s in range(rows):
        pos = jnp.where(rowi == s, lengths[s], pos)
    angle = pos.astype(F32) * freq
    cosv = jnp.cos(angle)
    sinv = jnp.sin(angle)

    def rotated(v, c, s):
        ln = lax.broadcasted_iota(jnp.int32, v.shape, 1)
        other = jnp.where(
            ln % ropew < half, -pltpu.roll(v, 128 - half, 1), pltpu.roll(v, half, 1)
        )
        return v * c + other * s

    pl.semaphore_wait(barrier, (n_tp - 1) + (n_ep - 1))
    local[0].wait()
    for d in near(n_z):
        to = 2 * lax.rem(place + d, n_z) + 1 - core
        hop(0, "tp", to, xo, xa.at[place]).start()
    shared = ((12, w1, (2, 3, 4)), (13, wku, (6,)), (14, wvu, (10,)), (15, wao, (11,)))
    for phase, held, waits in shared:
        for i in waits:
            local[i].wait()
        hop(phase, "tp", other, held.at[core], held.at[core]).start()

    local[1].wait()
    local[5].wait()
    tok = xo[...].astype(F32)
    own_normed = normed_rows(tok, again[...]).astype(BF16)
    krs[...] = jnp.zeros_like(krs)
    krs[:, 0:ropew] = nt(own_normed, wkr[...])
    new_rope = rotated(krs[...], cosv, sinv).astype(BF16).astype(F32)
    nrope_o[...] = new_rope[:, 0:ropew].astype(BF16)
    local[7].wait()

    await_line(0, xa)
    for phase, held, _ in shared[:2]:
        wait_bytes(recv.at[phase], held.at[0])
    half_rows = rows * n_z
    part = big.at[pl.ds(0, half_rows)]
    for z in range(n_z):
        big[pl.ds(rows * z, rows), :] = xa[z].astype(F32)
    normed = normed_rows(part[...], again[...]).astype(BF16)
    y = nt(normed, w1[...].reshape(-1, width))
    for k in range(2):
        yk = y[:, 128 * k : 128 * k + 128]
        ql = nn(yk[:, 0:nope].astype(BF16), wku[k])
        put(pl.ds(0, half_rows), jnp.concatenate([ql, yk], axis=1))
        for z in range(n_z):
            bs[z, :, wide * k : wide * (k + 1)] = get(pl.ds(rows * z, rows), wide).astype(BF16)
    to_line(2, bs, br)
    await_line(2, br)
    for t in range(n_tp):
        put(pl.ds(rows * t, rows), br[t // 2, :, wide * (t % 2) : wide * (t % 2 + 1)].astype(F32))

    parts = []
    ln4 = lax.broadcasted_iota(jnp.int32, (rows, 128), 1)
    per = 128 // latw
    for k in range(latent // 128):
        acc = jnp.zeros((rows, 128), F32)
        for j in range(per):
            t = k * per + j
            at = wide * (t % 2) + latent
            piece = br[t // 2, :, at : at + 128].astype(F32)
            shift = (j * latw - (nope + ropew)) % 128
            if shift:
                piece = pltpu.roll(piece, shift, 1)
            acc = jnp.where(ln4 // latw == j, piece, acc)
        parts.append(acc)
    latent_raw = jnp.concatenate(parts, axis=1)
    nl16 = normed_rows(latent_raw, lgain[...]).astype(BF16)
    nlat_o[...] = nl16
    new_latent = nl16.astype(F32)
    lane_r = lax.broadcasted_iota(jnp.int32, (rows, 128), 1)
    nr_al = jnp.where(
        (lane_r >= nope) & (lane_r < nope + ropew), pltpu.roll(new_rope, nope, 1), 0.0
    )

    local[8].wait()
    local[9].wait()
    n_heads = n_tp
    nlr = [new_latent[s : s + 1] for s in range(rows)]
    qrots, owns = [], []
    for s in range(rows):
        q = get(pl.ds(s, n_heads, stride=rows), latent)
        qr = rf[latent // 128, pl.ds(s, n_heads, stride=rows), :]
        sco[s] = nt(q.astype(BF16), cache[s])
        qrot = rotated(qr, cosv[s : s + 1], sinv[s : s + 1]).astype(BF16).astype(F32)
        owns.append(
            (
                jnp.sum(q * nlr[s], axis=-1, keepdims=True)
                + jnp.sum(qrot * nr_al[s : s + 1], axis=-1, keepdims=True)
            )
            * scale
        )
        shift = (ropew * s - nope) % 128
        lnq = lax.broadcasted_iota(jnp.int32, qrot.shape, 1)
        qrots.append(
            jnp.where(lnq // ropew == s, pltpu.roll(qrot, shift, 1) if shift else qrot, 0.0)
        )
    qrbd = jnp.concatenate(qrots, axis=0).astype(BF16)
    srope = nn(qrbd, rope[...])
    own_w = []
    for s in range(rows):
        sc = (sco[s] + srope[n_heads * s : n_heads * (s + 1)]) * scale
        col = lax.broadcasted_iota(jnp.int32, (n_heads, length), 1)
        sc = jnp.where(col < lengths[s], sc, -jnp.inf)
        own = owns[s]
        peak = jnp.maximum(jnp.max(sc, axis=-1, keepdims=True), own)
        pe = jnp.exp(sc - peak)
        oe = jnp.exp(own - peak)
        inv = 1.0 / (jnp.sum(pe, axis=-1, keepdims=True) + oe)
        prob[s] = (pe * inv).astype(BF16)
        own_w.append((oe * inv).astype(BF16).astype(F32))
    for s in range(rows):
        out = nn(prob[s], cache[s]) + own_w[s] * nlr[s]
        put(pl.ds(n_heads * s, n_heads), out)
    for t in range(n_tp):
        at = latent * (t % 2)
        cs[t // 2, :, at : at + latent] = get(pl.ds(t, rows, stride=n_heads), latent).astype(BF16)
    to_line(3, cs, cr)
    for i in range(12, 16):
        local[i].wait()

    cap = fs.shape[1]
    slots = n_ep * cap
    sl = lax.broadcasted_iota(jnp.int32, (slots, group), 0)
    want = (sl // cap) * n_tp + me
    hit = jnp.zeros((slots, group), F32)
    wgt = jnp.zeros((slots, group), F32)
    for k in range(ids_h.shape[0]):
        m = ids[k : k + 1, :] == want
        hit = jnp.where(m, 1.0, hit)
        wgt = jnp.where(m, rw[k : k + 1, :], wgt)
    before = (
        lax.broadcasted_iota(jnp.int32, (group, group), 0)
        < lax.broadcasted_iota(jnp.int32, (group, group), 1)
    )
    rank = nn(hit.astype(BF16), jnp.where(before, 1.0, 0.0).astype(BF16))
    taken = (hit > 0.5) & (jnp.abs(rank - (sl % cap).astype(F32)) < 0.5)
    disp = jnp.where(taken, 1.0, 0.0).astype(BF16)
    comb = jnp.where(taken, wgt, 0.0)
    comb_hi = comb.astype(BF16)
    comb_lo = (comb - comb_hi.astype(F32)).astype(BF16)

    await_line(3, cr)
    for phase, held, _ in shared[2:]:
        wait_bytes(recv.at[phase], held.at[0])
    total = None
    for k in range(2):
        for z in range(n_z):
            put(pl.ds(rows * z, rows), cr[z, :, latent * k : latent * (k + 1)].astype(F32))
        hv = nt(get(pl.ds(0, half_rows), latent).astype(BF16), wvu[k]).astype(BF16)
        term = nn(hv, wao[k])
        total = term if total is None else total + term
    part[...] = total
    for z in range(n_z):
        ds_[z] = big[pl.ds(rows * z, rows), :].astype(BF16)
    to_line(4, ds_, dr)
    for i in range(16, 25):
        local[i].wait()
    await_line(4, dr)
    after = tok + line_sum(dr)
    ee[core, place] = normed_rows(after, fgain[...]).astype(BF16)
    gather(6, 0, ee)
    gather_rest(6, 0, ee)
    for t in range(n_tp):
        big[pl.ds(rows * t, rows), :] = ee[t % 2, t // 2].astype(F32)
    ffn = big[...].astype(BF16)
    out = nn(disp, ffn)
    gate = bg[...].astype(F32)
    dots = big[:, 0:128] * gate[0:1]
    for k in range(1, width // 128):
        dots = dots + big[:, 128 * k : 128 * k + 128] * gate[k : k + 1]
    mix = jax.nn.sigmoid(jnp.sum(dots, axis=-1, keepdims=True))
    small[...] = out
    for g in range(n_ep):
        fs[g] = small[pl.ds(cap * g, cap), :].astype(BF16)
    to_all_ep(8, fs, fr)
    h = nt(ffn, w2[...])
    a, b = sg_h.shape[0], dg_h.shape[0]
    sact = (silu(h[:, 0:a]) * h[:, a : 2 * a]).astype(BF16)
    dact = (silu(h[:, 2 * a : 2 * a + b]) * h[:, 2 * a + b : 2 * a + 2 * b]).astype(BF16)
    await_all(8, n_ep, fr)
    for g in range(n_ep):
        small[pl.ds(cap * g, cap), :] = fr[g].astype(F32)
    arrived = small[...].astype(BF16)
    act = (silu(nn(arrived, eg[...])) * nn(arrived, eu[...])).astype(BF16)
    small[...] = nn(act, ed[...])
    for g in range(n_ep):
        gs[g] = small[pl.ds(cap * g, cap), :].astype(BF16)
    to_all_ep(9, gs, gr)
    big[...] = nn(sact, sd[...]) + mix * nn(dact, dd[...])
    await_all(9, n_ep, gr)
    for g in range(n_ep):
        small[pl.ds(cap * g, cap), :] = gr[g].astype(F32)
    back = small[...].astype(BF16)
    big[...] += tn(comb_hi, back) + tn(comb_lo, back)
    for t in range(n_tp):
        hs[t % 2, t // 2] = big[pl.ds(rows * t, rows), :].astype(BF16)
    reduce_start(10, 1, hs, hp)
    reduce_rest(10, 1, hs, hp, hm, hr)
    wait_bytes(send.at[6], ee.at[0, pl.ds(0, n_z - 1)])
    wait_bytes(send.at[7], ee.at[0])
    for phase, buf in ((0, xa), (2, bs), (3, cs), (4, ds_)):
        wait_bytes(send.at[phase], buf)
    for phase, buf in ((8, fs), (9, gs)):
        wait_bytes(send.at[phase], buf.at[pl.ds(0, n_ep - 1)])
    wait_bytes(send.at[10], hp)
    for phase, held, _ in shared:
        wait_bytes(send.at[phase], held.at[0])
    total = reduce_sum(10, hr)
    mixed_o[...] = (after + total).astype(BF16)
    wait_bytes(send.at[11], hm.at[pl.ds(0, n_z - 1)])


def local(
    tokens,
    lengths,
    cache_latent,
    cache_rope_key,
    route_ids,
    route_weights,
    attn_gain,
    w_query_nope,
    w_query_rope,
    w_latent_down,
    w_key_rope,
    latent_gain,
    w_key_up,
    w_value_up,
    w_attn_out,
    ffn_gain,
    expert_gate,
    expert_up,
    expert_down,
    shared_gate,
    shared_up,
    shared_down,
    dense_gate,
    dense_up,
    dense_down,
    branch_gate,
):
    n_tp = lax.axis_size("tp")
    n_ep = lax.axis_size("ep")
    rows, width = tokens.shape
    group = rows * n_tp
    wqn = w_query_nope.reshape(width, -1).T
    wqr = w_query_rope.reshape(width, -1).T
    wld = w_latent_down.T
    wkr = w_key_rope.T
    wku = w_key_up.reshape(w_key_up.shape[0], -1).T
    wvu = w_value_up.reshape(w_value_up.shape[0], -1).T
    wao = w_attn_out.reshape(-1, width)
    sg, su, dg, du = shared_gate.T, shared_up.T, dense_gate.T, dense_up.T
    rope = jnp.swapaxes(cache_rope_key, 1, 2).reshape(-1, cache_rope_key.shape[1])
    latent = wku.shape[1]
    ropew = wqr.shape[0]
    cap = max(2, -(-2 * rows * route_ids.shape[1] // n_ep))
    args = [
        lengths,
        tokens,
        cache_latent,
        rope,
        route_ids.T,
        route_weights.T,
        attn_gain.reshape(1, -1),
        wqn,
        wqr,
        wld,
        wkr,
        latent_gain.reshape(1, -1),
        wku,
        wvu,
        wao,
        ffn_gain.reshape(1, -1),
        expert_gate[0],
        expert_up[0],
        expert_down[0],
        sg,
        su,
        shared_down,
        dg,
        du,
        dense_down,
        branch_gate.reshape(-1, 128),
    ]
    hbm_spec = pl.BlockSpec(memory_space=pltpu.HBM)
    vm = lambda a: pltpu.VMEM(a.shape, a.dtype)
    n1 = wqn.shape[0] + ropew + wld.shape[0]
    n2 = 2 * (sg.shape[0] + dg.shape[0])
    wide = latent + 128
    scratch = [
        pltpu.SMEM(lengths.shape, jnp.int32),
        vm(cache_latent),
        vm(rope),
        vm(args[4]),
        vm(args[5]),
        vm(args[6]),
        pltpu.VMEM((2, n1, width), BF16),
        vm(wkr),
        vm(args[11]),
        pltpu.VMEM((2, *wku.shape), BF16),
        pltpu.VMEM((2, *wvu.shape), BF16),
        pltpu.VMEM((2, *wao.shape), BF16),
        vm(args[15]),
        vm(args[16]),
        vm(args[17]),
        vm(args[18]),
        pltpu.VMEM((n2, width), BF16),
        vm(shared_down),
        vm(dense_down),
        vm(args[25]),
        pltpu.VMEM((rows, width), BF16),
        pltpu.VMEM((n_tp // 2, rows, width), BF16),
        pltpu.VMEM((n_tp // 2, rows, 2 * wide), BF16),
        pltpu.VMEM((n_tp // 2, rows, 2 * wide), BF16),
        pltpu.VMEM((n_tp // 2, rows, 2 * latent), BF16),
        pltpu.VMEM((n_tp // 2, rows, 2 * latent), BF16),
        pltpu.VMEM((n_tp // 2, rows, width), BF16),
        pltpu.VMEM((n_tp // 2, rows, width), BF16),
        pltpu.VMEM((2, n_tp // 2, rows, width), BF16),
        pltpu.VMEM((n_ep, cap, width), BF16),
        pltpu.VMEM((n_ep, cap, width), BF16),
        pltpu.VMEM((n_ep, cap, width), BF16),
        pltpu.VMEM((n_ep, cap, width), BF16),
        pltpu.VMEM((2, n_tp // 2, rows, width), BF16),
        pltpu.VMEM((n_tp // 2, rows, width), BF16),
        pltpu.VMEM((n_tp // 2, rows, width), BF16),
        pltpu.VMEM((n_tp // 2, rows, width), BF16),
        pltpu.VMEM((rows, n_tp, cache_latent.shape[1]), F32),
        pltpu.VMEM((rows, n_tp, cache_latent.shape[1]), BF16),
        pltpu.VMEM((group, width), F32),
        pltpu.VMEM((n_ep * cap, width), F32),
        pltpu.VMEM((wide // 128, group, 128), F32),
        pltpu.VMEM((rows, 128), F32),
        pltpu.SemaphoreType.DMA((26,)),
        pltpu.SemaphoreType.DMA((16,)),
        pltpu.SemaphoreType.DMA((16,)),
        pltpu.SemaphoreType.DMA((2, n_tp // 2)),
    ]
    found = pl.pallas_call(
        functools.partial(layer_kernel, n_tp, n_ep),
        out_shape=(
            jax.ShapeDtypeStruct((rows, width), BF16),
            jax.ShapeDtypeStruct((rows, latent), BF16),
            jax.ShapeDtypeStruct((rows, ropew), BF16),
        ),
        in_specs=[hbm_spec] * 26,
        out_specs=(pl.BlockSpec(memory_space=pltpu.VMEM),) * 3,
        scratch_shapes=scratch,
        compiler_params=pltpu.CompilerParams(
            collective_id=0, has_side_effects=True, vmem_limit_bytes=40 * 1024 * 1024
        ),
        name="layer",
    )(*[pltpu.with_memory_space_constraint(a, pltpu.HBM) for a in args])
    vmem = pl.BlockSpec(memory_space=pltpu.VMEM)
    return pl.pallas_call(
        finish_kernel,
        out_shape=tuple(jax.ShapeDtypeStruct(a.shape, a.dtype) for a in found),
        in_specs=[vmem] * 3,
        out_specs=(vmem,) * 3,
        compiler_params=pltpu.CompilerParams(vmem_limit_bytes=8 * 1024 * 1024),
        name="finish",
    )(*found)


def solution(mesh):
    in_specs = (
        P(("ep", "tp"), None),
        P(("ep", "tp")),
        P(("ep", "tp"), None, None),
        P(("ep", "tp"), None, None),
        P("ep", None),
        P("ep", None),
        P(),
        P(None, "tp", None),
        P(None, "tp", None),
        P(None, "tp"),
        P(),
        P(),
        P(None, "tp", None),
        P(None, "tp", None),
        P("tp", None, None),
        P(),
        P(("ep", "tp"), None, None),
        P(("ep", "tp"), None, None),
        P(("ep", "tp"), None, None),
        P(None, "tp"),
        P(None, "tp"),
        P("tp", None),
        P(None, "tp"),
        P(None, "tp"),
        P("tp", None),
        P(),
    )
    out_specs = (P(("ep", "tp"), None), P(("ep", "tp"), None), P(("ep", "tp"), None))
    return jax.shard_map(local, mesh=mesh, in_specs=in_specs, out_specs=out_specs, check_vma=False)
```

```python
import functools

import jax
import jax.numpy as jnp
from jax import lax
from jax.experimental import pallas as pl
from jax.experimental.pallas import tpu as pltpu
from jax.sharding import PartitionSpec as P

EPS = 1e-06
ROPE_BASE = 10000.0
MESH = pl.DeviceIdType.MESH
F32 = jnp.float32
BF16 = jnp.bfloat16


def nn(a, b):
    return lax.dot_general(a, b, (((1,), (0,)), ((), ())), preferred_element_type=F32)


def nt(a, b):
    return lax.dot_general(a, b, (((1,), (1,)), ((), ())), preferred_element_type=F32)


def tn(a, b):
    return lax.dot_general(a, b, (((0,), (0,)), ((), ())), preferred_element_type=F32)


def normed_rows(x, gain):
    return x * lax.rsqrt(jnp.mean(x * x, axis=-1, keepdims=True) + EPS) * gain


def silu(v):
    return v / (1.0 + jnp.exp(-v))


def finish_kernel(mixed, nlat, nrope, mixed_o, nlat_o, nrope_o):
    mixed_o[...] = mixed[...]
    nlat_o[...] = nlat[...]
    nrope_o[...] = nrope[...]


def layer_kernel(
    n_tp,
    n_ep,
    lengths_h,
    tokens,
    cache_h,
    rope_h,
    ids_h,
    rw_h,
    again_h,
    wqn_h,
    wqr_h,
    wld_h,
    wkr_h,
    lgain_h,
    wku_h,
    wvu_h,
    wao_h,
    fgain_h,
    eg_h,
    eu_h,
    ed_h,
    sg_h,
    su_h,
    sd_h,
    dg_h,
    du_h,
    dd_h,
    bg_h,
    mixed_o,
    nlat_o,
    nrope_o,
    lengths,
    cache,
    rope,
    ids,
    rw,
    again,
    w1,
    wkr,
    lgain,
    wku,
    wvu,
    wao,
    fgain,
    eg,
    eu,
    ed,
    w2,
    sd,
    dd,
    bg,
    xo,
    xa,
    bs,
    br,
    cs,
    cr,
    ds_,
    dr,
    ee,
    fs,
    fr,
    gs,
    gr,
    hs,
    hp,
    hm,
    hr,
    sco,
    prob,
    big,
    small,
    rf,
    krs,
    lsem,
    send,
    recv,
    each,
):
    me = lax.axis_index("tp")
    grp = lax.axis_index("ep")
    rows, width = tokens.shape
    group = rows * n_tp
    nope = wqn_h.shape[0]
    ropew = wqr_h.shape[0]
    latw = wld_h.shape[0]
    latent = wku_h.shape[1]
    length = cache.shape[1]
    scale = (nope + ropew) ** (-0.5)

    wide = latent + 128
    n_z = n_tp // 2
    core = lax.rem(me, 2)
    place = lax.div(me, 2)
    other = 2 * place + 1 - core

    def put(where, value):
        for k in range(value.shape[1] // 128):
            rf[k, where, :] = value[:, 128 * k : 128 * k + 128]

    def get(where, columns):
        return jnp.concatenate([rf[k, where, :] for k in range(columns // 128)], axis=1)

    jobs = [
        (tokens, xo),
        (again_h, again),
        (wqn_h, w1.at[core, pl.ds(0, nope)]),
        (wqr_h, w1.at[core, pl.ds(nope, ropew)]),
        (wld_h, w1.at[core, pl.ds(nope + ropew, latw)]),
        (wkr_h, wkr),
        (wku_h, wku.at[core]),
        (lgain_h, lgain),
        (cache_h, cache),
        (rope_h, rope),
        (wvu_h, wvu.at[core]),
        (wao_h, wao.at[core]),
        (fgain_h, fgain),
        (ids_h, ids),
        (rw_h, rw),
        (bg_h, bg),
        (sg_h, w2.at[pl.ds(0, sg_h.shape[0])]),
        (su_h, w2.at[pl.ds(sg_h.shape[0], sg_h.shape[0])]),
        (dg_h, w2.at[pl.ds(2 * sg_h.shape[0], dg_h.shape[0])]),
        (du_h, w2.at[pl.ds(2 * sg_h.shape[0] + dg_h.shape[0], dg_h.shape[0])]),
        (eg_h, eg),
        (eu_h, eu),
        (ed_h, ed),
        (sd_h, sd),
        (dd_h, dd),
        (lengths_h, lengths),
    ]
    local = [pltpu.make_async_copy(s, d, lsem.at[i]) for i, (s, d) in enumerate(jobs)]
    barrier = pltpu.get_barrier_semaphore()

    def near(n):
        return sorted(range(n), key=lambda d: (-min(d, n - d), d))

    for d in near(n_z):
        for k in range(2):
            if d or k:
                to = 2 * lax.rem(place + d, n_z) + lax.rem(core + k, 2)
                pl.semaphore_signal(barrier, inc=1, device_id={"tp": to}, device_id_type=MESH)
    for d in near(n_ep):
        if d:
            to = lax.rem(grp + d, n_ep)
            pl.semaphore_signal(barrier, inc=1, device_id={"ep": to, "tp": other}, device_id_type=MESH)
    for c in local:
        c.start()

    def hop(phase, axis, to, src, dst, got=None):
        return pltpu.make_async_remote_copy(
            src_ref=src,
            dst_ref=dst,
            send_sem=send.at[phase],
            recv_sem=recv.at[phase] if got is None else got,
            device_id={axis: to, "tp": other} if axis == "ep" else {axis: to},
            device_id_type=MESH,
        )

    def wait_bytes(sem, like):
        pltpu.make_async_copy(like, like, sem).wait()

    def to_line(phase, src, dst):
        for d in near(n_z):
            z = lax.rem(place + d, n_z)
            hop(phase, "tp", 2 * z + 1 - core, src.at[z], dst.at[place]).start()

    def await_line(phase, dst):
        wait_bytes(recv.at[phase], dst)

    side = int(n_ep**0.5)
    side = side if side * side == n_ep else 1
    across = n_ep // side

    def to_all_ep(phase, src, dst):
        y, x = lax.div(grp, across), lax.rem(grp, across)
        offsets = [(dy, dx) for dy in range(side) for dx in range(across)]
        offsets.sort(key=lambda o: -min(o[0], side - o[0]) - min(o[1], across - o[1]))
        for dy, dx in offsets:
            to = lax.rem(y + dy, side) * across + lax.rem(x + dx, across)
            hop(phase, "ep", to, src.at[to], dst.at[grp]).start()

    def await_all(phase, n, dst):
        wait_bytes(recv.at[phase], dst.at[pl.ds(0, n - 1)])


    def gather(phase, row, buf):
        own = buf.at[core, place]
        for d in near(n_z):
            if d:
                z = lax.rem(place + d, n_z)
                hop(phase, "tp", 2 * z + core, own, own, each.at[row, d]).start()
        hop(phase + 1, "tp", other, own, own).start()

    def gather_rest(phase, row, buf):
        for d in near(n_z):
            if d:
                block = buf.at[core, lax.rem(place + n_z - d, n_z)]
                wait_bytes(each.at[row, d], block)
                hop(phase + 1, "tp", other, block, block).start()
        wait_bytes(recv.at[phase + 1], buf.at[0])

    def line_sum(dst):
        total = dst[0].astype(F32)
        for z in range(1, n_z):
            total = total + dst[z].astype(F32)
        return total

    local[25].wait()
    lane = lax.broadcasted_iota(jnp.int32, (rows, 128), 1)
    rowi = lax.broadcasted_iota(jnp.int32, (rows, 128), 0)
    half = ropew // 2
    freq = jnp.zeros((rows, 128), F32)
    for i in range(half):
        freq = jnp.where(lane % half == i, F32(ROPE_BASE ** (-i / half)), freq)
    pos = jnp.zeros((rows, 128), jnp.int32)
    for s in range(rows):
        pos = jnp.where(rowi == s, lengths[s], pos)
    angle = pos.astype(F32) * freq
    cosv = jnp.cos(angle)
    sinv = jnp.sin(angle)

    def rotated(v, c, s):
        ln = lax.broadcasted_iota(jnp.int32, v.shape, 1)
        other = jnp.where(
            ln % ropew < half, -pltpu.roll(v, 128 - half, 1), pltpu.roll(v, half, 1)
        )
        return v * c + other * s

    pl.semaphore_wait(barrier, (n_tp - 1) + (n_ep - 1))
    local[0].wait()
    for d in near(n_z):
        to = 2 * lax.rem(place + d, n_z) + 1 - core
        hop(0, "tp", to, xo, xa.at[place]).start()
    shared = ((12, w1, (2, 3, 4)), (13, wku, (6,)), (14, wvu, (10,)), (15, wao, (11,)))

    def share(parts):
        for phase, held, waits in parts:
            for i in waits:
                local[i].wait()
            hop(phase, "tp", other, held.at[core], held.at[core]).start()

    share(shared[:2])

    local[1].wait()
    local[5].wait()
    tok = xo[...].astype(F32)
    own_normed = normed_rows(tok, again[...]).astype(BF16)
    krs[...] = jnp.zeros_like(krs)
    krs[:, 0:ropew] = nt(own_normed, wkr[...])
    new_rope = rotated(krs[...], cosv, sinv).astype(BF16).astype(F32)
    nrope_o[...] = new_rope[:, 0:ropew].astype(BF16)
    local[7].wait()

    await_line(0, xa)
    for phase, held, _ in shared[:2]:
        wait_bytes(recv.at[phase], held.at[0])
    half_rows = rows * n_z
    part = big.at[pl.ds(0, half_rows)]
    for z in range(n_z):
        big[pl.ds(rows * z, rows), :] = xa[z].astype(F32)
    normed = normed_rows(part[...], again[...]).astype(BF16)
    y = nt(normed, w1[...].reshape(-1, width))
    for k in range(2):
        yk = y[:, 128 * k : 128 * k + 128]
        ql = nn(yk[:, 0:nope].astype(BF16), wku[k])
        put(pl.ds(0, half_rows), jnp.concatenate([ql, yk], axis=1))
        for z in range(n_z):
            bs[z, :, wide * k : wide * (k + 1)] = get(pl.ds(rows * z, rows), wide).astype(BF16)
    to_line(2, bs, br)
    share(shared[2:])
    local[8].wait()
    local[9].wait()
    await_line(2, br)
    for t in range(n_tp):
        put(pl.ds(rows * t, rows), br[t // 2, :, wide * (t % 2) : wide * (t % 2 + 1)].astype(F32))

    parts = []
    ln4 = lax.broadcasted_iota(jnp.int32, (rows, 128), 1)
    per = 128 // latw
    for k in range(latent // 128):
        acc = jnp.zeros((rows, 128), F32)
        for j in range(per):
            t = k * per + j
            at = wide * (t % 2) + latent
            piece = br[t // 2, :, at : at + 128].astype(F32)
            shift = (j * latw - (nope + ropew)) % 128
            if shift:
                piece = pltpu.roll(piece, shift, 1)
            acc = jnp.where(ln4 // latw == j, piece, acc)
        parts.append(acc)
    latent_raw = jnp.concatenate(parts, axis=1)
    nl16 = normed_rows(latent_raw, lgain[...]).astype(BF16)
    nlat_o[...] = nl16
    new_latent = nl16.astype(F32)
    lane_r = lax.broadcasted_iota(jnp.int32, (rows, 128), 1)
    nr_al = jnp.where(
        (lane_r >= nope) & (lane_r < nope + ropew), pltpu.roll(new_rope, nope, 1), 0.0
    )

    n_heads = n_tp
    nlr = [new_latent[s : s + 1] for s in range(rows)]
    qrots, owns = [], []
    for s in range(rows):
        q = get(pl.ds(s, n_heads, stride=rows), latent)
        qr = rf[latent // 128, pl.ds(s, n_heads, stride=rows), :]
        sco[s] = nt(q.astype(BF16), cache[s])
        qrot = rotated(qr, cosv[s : s + 1], sinv[s : s + 1]).astype(BF16).astype(F32)
        owns.append(
            (
                jnp.sum(q * nlr[s], axis=-1, keepdims=True)
                + jnp.sum(qrot * nr_al[s : s + 1], axis=-1, keepdims=True)
            )
            * scale
        )
        shift = (ropew * s - nope) % 128
        lnq = lax.broadcasted_iota(jnp.int32, qrot.shape, 1)
        qrots.append(
            jnp.where(lnq // ropew == s, pltpu.roll(qrot, shift, 1) if shift else qrot, 0.0)
        )
    qrbd = jnp.concatenate(qrots, axis=0).astype(BF16)
    srope = nn(qrbd, rope[...])
    own_w = []
    for s in range(rows):
        sc = (sco[s] + srope[n_heads * s : n_heads * (s + 1)]) * scale
        col = lax.broadcasted_iota(jnp.int32, (n_heads, length), 1)
        sc = jnp.where(col < lengths[s], sc, -jnp.inf)
        own = owns[s]
        peak = jnp.maximum(jnp.max(sc, axis=-1, keepdims=True), own)
        pe = jnp.exp(sc - peak)
        oe = jnp.exp(own - peak)
        inv = 1.0 / (jnp.sum(pe, axis=-1, keepdims=True) + oe)
        prob[s] = (pe * inv).astype(BF16)
        own_w.append((oe * inv).astype(BF16).astype(F32))
    for s in range(rows):
        out = nn(prob[s], cache[s]) + own_w[s] * nlr[s]
        put(pl.ds(n_heads * s, n_heads), out)
    for t in range(n_tp):
        at = latent * (t % 2)
        cs[t // 2, :, at : at + latent] = get(pl.ds(t, rows, stride=n_heads), latent).astype(BF16)
    to_line(3, cs, cr)
    for i in range(12, 16):
        local[i].wait()

    cap = fs.shape[1]
    slots = n_ep * cap
    sl = lax.broadcasted_iota(jnp.int32, (slots, group), 0)
    want = (sl // cap) * n_tp + other
    hit = jnp.zeros((slots, group), F32)
    wgt = jnp.zeros((slots, group), F32)
    for k in range(ids_h.shape[0]):
        m = ids[k : k + 1, :] == want
        hit = jnp.where(m, 1.0, hit)
        wgt = jnp.where(m, rw[k : k + 1, :], wgt)
    before = (
        lax.broadcasted_iota(jnp.int32, (group, group), 0)
        < lax.broadcasted_iota(jnp.int32, (group, group), 1)
    )
    rank = nn(hit.astype(BF16), jnp.where(before, 1.0, 0.0).astype(BF16))
    taken = (hit > 0.5) & (jnp.abs(rank - (sl % cap).astype(F32)) < 0.5)
    disp = jnp.where(taken, 1.0, 0.0).astype(BF16)
    comb = jnp.where(taken, wgt, 0.0)
    comb_hi = comb.astype(BF16)
    comb_lo = (comb - comb_hi.astype(F32)).astype(BF16)

    await_line(3, cr)
    for phase, held, _ in shared[2:]:
        wait_bytes(recv.at[phase], held.at[0])
    total = None
    for k in range(2):
        for z in range(n_z):
            put(pl.ds(rows * z, rows), cr[z, :, latent * k : latent * (k + 1)].astype(F32))
        hv = nt(get(pl.ds(0, half_rows), latent).astype(BF16), wvu[k]).astype(BF16)
        term = nn(hv, wao[k])
        total = term if total is None else total + term
    part[...] = total
    for z in range(n_z):
        ds_[z] = big[pl.ds(rows * z, rows), :].astype(BF16)
    to_line(4, ds_, dr)
    for i in range(16, 25):
        local[i].wait()
    await_line(4, dr)
    after = tok + line_sum(dr)
    ee[core, place] = normed_rows(after, fgain[...]).astype(BF16)
    gather(6, 0, ee)
    gather_rest(6, 0, ee)
    for t in range(n_tp):
        big[pl.ds(rows * t, rows), :] = ee[t % 2, t // 2].astype(F32)
    ffn = big[...].astype(BF16)
    out = nn(disp, ffn)
    small[...] = out
    for g in range(n_ep):
        fs[g] = small[pl.ds(cap * g, cap), :].astype(BF16)
    to_all_ep(8, fs, fr)
    gate = bg[...].astype(F32)
    dots = big[:, 0:128] * gate[0:1]
    for k in range(1, width // 128):
        dots = dots + big[:, 128 * k : 128 * k + 128] * gate[k : k + 1]
    mix = jax.nn.sigmoid(jnp.sum(dots, axis=-1, keepdims=True))
    h = nt(ffn, w2[...])
    a, b = sg_h.shape[0], dg_h.shape[0]
    sact = (silu(h[:, 0:a]) * h[:, a : 2 * a]).astype(BF16)
    dact = (silu(h[:, 2 * a : 2 * a + b]) * h[:, 2 * a + b : 2 * a + 2 * b]).astype(BF16)
    wait_bytes(recv.at[8], fr)
    for g in range(n_ep):
        small[pl.ds(cap * g, cap), :] = fr[g].astype(F32)
    arrived = small[...].astype(BF16)
    act = (silu(nn(arrived, eg[...])) * nn(arrived, eu[...])).astype(BF16)
    small[...] = nn(act, ed[...])
    for g in range(n_ep):
        gs[g] = small[pl.ds(cap * g, cap), :].astype(BF16)
    to_all_ep(9, gs, gr)
    big[...] = nn(sact, sd[...]) + mix * nn(dact, dd[...])
    wait_bytes(recv.at[9], gr)
    for g in range(n_ep):
        small[pl.ds(cap * g, cap), :] = gr[g].astype(F32)
    back = small[...].astype(BF16)
    big[...] += tn(comb_hi, back) + tn(comb_lo, back)
    def two(z):
        both = big[pl.ds(pl.multiple_of(2 * rows * z, 2 * rows), 2 * rows), :]
        low, high = both[0:rows], both[rows : 2 * rows]
        return jnp.where(core == 0, low, high), jnp.where(core == 0, high, low)

    order = [(d, lax.rem(place + d, n_z)) for d in near(n_z)]
    for d, z in order:
        hs[z] = two(z)[1].astype(BF16)
        hop(10, "tp", other, hs.at[z], hp.at[z], each.at[1, d]).start()
    for d, z in order:
        wait_bytes(each.at[1, d], hp.at[z])
        hm[z] = (two(z)[0] + hp[z].astype(F32)).astype(BF16)
        if d:
            hop(11, "tp", 2 * z + core, hm.at[z], hr.at[place]).start()
        else:
            hr[place] = hm[z]
    wait_bytes(send.at[6], ee.at[0, pl.ds(0, n_z - 1)])
    wait_bytes(send.at[7], ee.at[0])
    for phase, buf in ((0, xa), (2, bs), (3, cs), (4, ds_)):
        wait_bytes(send.at[phase], buf)
    for phase, buf in ((8, fs), (9, gs)):
        wait_bytes(send.at[phase], buf)
    wait_bytes(send.at[10], hp)
    for phase, held, _ in shared:
        wait_bytes(send.at[phase], held.at[0])
    wait_bytes(recv.at[11], hr.at[pl.ds(0, n_z - 1)])
    total = line_sum(hr)
    mixed_o[...] = (after + total).astype(BF16)
    wait_bytes(send.at[11], hm.at[pl.ds(0, n_z - 1)])


def local(
    tokens,
    lengths,
    cache_latent,
    cache_rope_key,
    route_ids,
    route_weights,
    attn_gain,
    w_query_nope,
    w_query_rope,
    w_latent_down,
    w_key_rope,
    latent_gain,
    w_key_up,
    w_value_up,
    w_attn_out,
    ffn_gain,
    expert_gate,
    expert_up,
    expert_down,
    shared_gate,
    shared_up,
    shared_down,
    dense_gate,
    dense_up,
    dense_down,
    branch_gate,
):
    n_tp = lax.axis_size("tp")
    n_ep = lax.axis_size("ep")
    rows, width = tokens.shape
    group = rows * n_tp
    wqn = w_query_nope.reshape(width, -1).T
    wqr = w_query_rope.reshape(width, -1).T
    wld = w_latent_down.T
    wkr = w_key_rope.T
    wku = w_key_up.reshape(w_key_up.shape[0], -1).T
    wvu = w_value_up.reshape(w_value_up.shape[0], -1).T
    wao = w_attn_out.reshape(-1, width)
    sg, su, dg, du = shared_gate.T, shared_up.T, dense_gate.T, dense_up.T
    rope = jnp.swapaxes(cache_rope_key, 1, 2).reshape(-1, cache_rope_key.shape[1])
    latent = wku.shape[1]
    ropew = wqr.shape[0]
    cap = max(2, -(-2 * rows * route_ids.shape[1] // n_ep))
    args = [
        lengths,
        tokens,
        cache_latent,
        rope,
        route_ids.T,
        route_weights.T,
        attn_gain.reshape(1, -1),
        wqn,
        wqr,
        wld,
        wkr,
        latent_gain.reshape(1, -1),
        wku,
        wvu,
        wao,
        ffn_gain.reshape(1, -1),
        expert_gate[0],
        expert_up[0],
        expert_down[0],
        sg,
        su,
        shared_down,
        dg,
        du,
        dense_down,
        branch_gate.reshape(-1, 128),
    ]
    hbm_spec = pl.BlockSpec(memory_space=pltpu.HBM)
    vm = lambda a: pltpu.VMEM(a.shape, a.dtype)
    n1 = wqn.shape[0] + ropew + wld.shape[0]
    n2 = 2 * (sg.shape[0] + dg.shape[0])
    wide = latent + 128
    scratch = [
        pltpu.SMEM(lengths.shape, jnp.int32),
        vm(cache_latent),
        vm(rope),
        vm(args[4]),
        vm(args[5]),
        vm(args[6]),
        pltpu.VMEM((2, n1, width), BF16),
        vm(wkr),
        vm(args[11]),
        pltpu.VMEM((2, *wku.shape), BF16),
        pltpu.VMEM((2, *wvu.shape), BF16),
        pltpu.VMEM((2, *wao.shape), BF16),
        vm(args[15]),
        vm(args[16]),
        vm(args[17]),
        vm(args[18]),
        pltpu.VMEM((n2, width), BF16),
        vm(shared_down),
        vm(dense_down),
        vm(args[25]),
        pltpu.VMEM((rows, width), BF16),
        pltpu.VMEM((n_tp // 2, rows, width), BF16),
        pltpu.VMEM((n_tp // 2, rows, 2 * wide), BF16),
        pltpu.VMEM((n_tp // 2, rows, 2 * wide), BF16),
        pltpu.VMEM((n_tp // 2, rows, 2 * latent), BF16),
        pltpu.VMEM((n_tp // 2, rows, 2 * latent), BF16),
        pltpu.VMEM((n_tp // 2, rows, width), BF16),
        pltpu.VMEM((n_tp // 2, rows, width), BF16),
        pltpu.VMEM((2, n_tp // 2, rows, width), BF16),
        pltpu.VMEM((n_ep, cap, width), BF16),
        pltpu.VMEM((n_ep, cap, width), BF16),
        pltpu.VMEM((n_ep, cap, width), BF16),
        pltpu.VMEM((n_ep, cap, width), BF16),
        pltpu.VMEM((n_tp // 2, rows, width), BF16),
        pltpu.VMEM((n_tp // 2, rows, width), BF16),
        pltpu.VMEM((n_tp // 2, rows, width), BF16),
        pltpu.VMEM((n_tp // 2, rows, width), BF16),
        pltpu.VMEM((rows, n_tp, cache_latent.shape[1]), F32),
        pltpu.VMEM((rows, n_tp, cache_latent.shape[1]), BF16),
        pltpu.VMEM((group, width), F32),
        pltpu.VMEM((n_ep * cap, width), F32),
        pltpu.VMEM((wide // 128, group, 128), F32),
        pltpu.VMEM((rows, 128), F32),
        pltpu.SemaphoreType.DMA((26,)),
        pltpu.SemaphoreType.DMA((16,)),
        pltpu.SemaphoreType.DMA((16,)),
        pltpu.SemaphoreType.DMA((2, n_tp // 2)),
    ]
    found = pl.pallas_call(
        functools.partial(layer_kernel, n_tp, n_ep),
        out_shape=(
            jax.ShapeDtypeStruct((rows, width), BF16),
            jax.ShapeDtypeStruct((rows, latent), BF16),
            jax.ShapeDtypeStruct((rows, ropew), BF16),
        ),
        in_specs=[hbm_spec] * 26,
        out_specs=(pl.BlockSpec(memory_space=pltpu.VMEM),) * 3,
        scratch_shapes=scratch,
        compiler_params=pltpu.CompilerParams(
            collective_id=0, has_side_effects=True, vmem_limit_bytes=40 * 1024 * 1024
        ),
        name="layer",
    )(*[pltpu.with_memory_space_constraint(a, pltpu.HBM) for a in args])
    vmem = pl.BlockSpec(memory_space=pltpu.VMEM)
    return pl.pallas_call(
        finish_kernel,
        out_shape=tuple(jax.ShapeDtypeStruct(a.shape, a.dtype) for a in found),
        in_specs=[vmem] * 3,
        out_specs=(vmem,) * 3,
        compiler_params=pltpu.CompilerParams(vmem_limit_bytes=8 * 1024 * 1024),
        name="finish",
    )(*found)


def solution(mesh):
    in_specs = (
        P(("ep", "tp"), None),
        P(("ep", "tp")),
        P(("ep", "tp"), None, None),
        P(("ep", "tp"), None, None),
        P("ep", None),
        P("ep", None),
        P(),
        P(None, "tp", None),
        P(None, "tp", None),
        P(None, "tp"),
        P(),
        P(),
        P(None, "tp", None),
        P(None, "tp", None),
        P("tp", None, None),
        P(),
        P(("ep", "tp"), None, None),
        P(("ep", "tp"), None, None),
        P(("ep", "tp"), None, None),
        P(None, "tp"),
        P(None, "tp"),
        P("tp", None),
        P(None, "tp"),
        P(None, "tp"),
        P("tp", None),
        P(),
    )
    out_specs = (P(("ep", "tp"), None), P(("ep", "tp"), None), P(("ep", "tp"), None))
    return jax.shard_map(local, mesh=mesh, in_specs=in_specs, out_specs=out_specs, check_vma=False)
```

```python
import functools

import jax
import jax.numpy as jnp
from jax import lax
from jax.experimental import pallas as pl
from jax.experimental.pallas import tpu as pltpu
from jax.sharding import PartitionSpec as P

EPS = 1e-06
ROPE_BASE = 10000.0
MESH = pl.DeviceIdType.MESH
F32 = jnp.float32
BF16 = jnp.bfloat16


def nn(a, b):
    return lax.dot_general(a, b, (((1,), (0,)), ((), ())), preferred_element_type=F32)


def nt(a, b):
    return lax.dot_general(a, b, (((1,), (1,)), ((), ())), preferred_element_type=F32)


def tn(a, b):
    return lax.dot_general(a, b, (((0,), (0,)), ((), ())), preferred_element_type=F32)


def normed_rows(x, gain):
    return x * lax.rsqrt(jnp.mean(x * x, axis=-1, keepdims=True) + EPS) * gain


def silu(v):
    return v / (1.0 + jnp.exp(-v))


def finish_kernel(mixed, nlat, nrope, mixed_o, nlat_o, nrope_o):
    mixed_o[...] = mixed[...]
    nlat_o[...] = nlat[...]
    nrope_o[...] = nrope[...]


def layer_kernel(
    n_tp,
    n_ep,
    lengths_h,
    tokens,
    cache_h,
    rope_h,
    ids_h,
    rw_h,
    again_h,
    wqn_h,
    wqr_h,
    wld_h,
    wkr_h,
    lgain_h,
    wku_h,
    wvu_h,
    wao_h,
    fgain_h,
    eg_h,
    eu_h,
    ed_h,
    sg_h,
    su_h,
    sd_h,
    dg_h,
    du_h,
    dd_h,
    bg_h,
    mixed_o,
    nlat_o,
    nrope_o,
    lengths,
    cache,
    rope,
    ids,
    rw,
    again,
    w1,
    wkr,
    lgain,
    wku,
    wvu,
    wao,
    fgain,
    eg,
    eu,
    ed,
    w2,
    sd,
    dd,
    bg,
    xo,
    xa,
    bs,
    br,
    cs,
    cr,
    ds_,
    dr,
    ee,
    fs,
    fr,
    gs,
    gr,
    hs,
    hp,
    hm,
    hr,
    sco,
    prob,
    big,
    small,
    rf,
    krs,
    lsem,
    send,
    recv,
    each,
):
    me = lax.axis_index("tp")
    grp = lax.axis_index("ep")
    rows, width = tokens.shape
    group = rows * n_tp
    nope = wqn_h.shape[0]
    ropew = wqr_h.shape[0]
    latw = wld_h.shape[0]
    latent = wku_h.shape[1]
    length = cache.shape[1]
    scale = (nope + ropew) ** (-0.5)

    wide = latent + 128
    n_z = n_tp // 2
    core = lax.rem(me, 2)
    place = lax.div(me, 2)
    other = 2 * place + 1 - core

    def put(where, value):
        for k in range(value.shape[1] // 128):
            rf[k, where, :] = value[:, 128 * k : 128 * k + 128]

    def get(where, columns):
        return jnp.concatenate([rf[k, where, :] for k in range(columns // 128)], axis=1)

    jobs = [
        (tokens, xo),
        (again_h, again),
        (wqn_h, w1.at[core, pl.ds(0, nope)]),
        (wqr_h, w1.at[core, pl.ds(nope, ropew)]),
        (wld_h, w1.at[core, pl.ds(nope + ropew, latw)]),
        (wkr_h, wkr),
        (wku_h, wku.at[core]),
        (lgain_h, lgain),
        (cache_h, cache),
        (rope_h, rope),
        (wvu_h, wvu.at[core]),
        (wao_h, wao.at[core]),
        (fgain_h, fgain),
        (ids_h, ids),
        (rw_h, rw),
        (bg_h, bg),
        (sg_h, w2.at[pl.ds(0, sg_h.shape[0])]),
        (su_h, w2.at[pl.ds(sg_h.shape[0], sg_h.shape[0])]),
        (dg_h, w2.at[pl.ds(2 * sg_h.shape[0], dg_h.shape[0])]),
        (du_h, w2.at[pl.ds(2 * sg_h.shape[0] + dg_h.shape[0], dg_h.shape[0])]),
        (eg_h, eg),
        (eu_h, eu),
        (ed_h, ed),
        (sd_h, sd),
        (dd_h, dd),
        (lengths_h, lengths),
    ]
    local = [pltpu.make_async_copy(s, d, lsem.at[i]) for i, (s, d) in enumerate(jobs)]
    barrier = pltpu.get_barrier_semaphore()

    def near(n):
        return sorted(range(n), key=lambda d: (-min(d, n - d), d))

    for d in near(n_z):
        for k in range(2):
            if d or k:
                to = 2 * lax.rem(place + d, n_z) + lax.rem(core + k, 2)
                pl.semaphore_signal(barrier, inc=1, device_id={"tp": to}, device_id_type=MESH)
    for d in near(n_ep):
        if d:
            to = lax.rem(grp + d, n_ep)
            pl.semaphore_signal(barrier, inc=1, device_id={"ep": to, "tp": other}, device_id_type=MESH)
    for c in local:
        c.start()

    def hop(phase, axis, to, src, dst, got=None):
        return pltpu.make_async_remote_copy(
            src_ref=src,
            dst_ref=dst,
            send_sem=send.at[phase],
            recv_sem=recv.at[phase] if got is None else got,
            device_id={axis: to, "tp": other} if axis == "ep" else {axis: to},
            device_id_type=MESH,
        )

    def wait_bytes(sem, like):
        pltpu.make_async_copy(like, like, sem).wait()

    def to_line(phase, src, dst):
        for d in near(n_z):
            z = lax.rem(place + d, n_z)
            hop(phase, "tp", 2 * z + 1 - core, src.at[z], dst.at[place]).start()

    def await_line(phase, dst):
        wait_bytes(recv.at[phase], dst)

    side = int(n_ep**0.5)
    side = side if side * side == n_ep else 1
    across = n_ep // side

    def to_all_ep(phase, src, dst):
        y, x = lax.div(grp, across), lax.rem(grp, across)
        offsets = [(dy, dx) for dy in range(side) for dx in range(across)]
        offsets.sort(key=lambda o: -min(o[0], side - o[0]) - min(o[1], across - o[1]))
        for dy, dx in offsets:
            to = lax.rem(y + dy, side) * across + lax.rem(x + dx, across)
            hop(phase, "ep", to, src.at[to], dst.at[grp]).start()

    def await_all(phase, n, dst):
        wait_bytes(recv.at[phase], dst.at[pl.ds(0, n - 1)])


    def gather(phase, row, buf):
        own = buf.at[core, place]
        for d in near(n_z):
            if d:
                z = lax.rem(place + d, n_z)
                hop(phase, "tp", 2 * z + 1 - core, own, own, each.at[row, d]).start()
        hop(phase + 1, "tp", other, own, own).start()

    def gather_rest(phase, row, buf):
        for d in near(n_z):
            if d:
                block = buf.at[1 - core, lax.rem(place + n_z - d, n_z)]
                wait_bytes(each.at[row, d], block)
                hop(phase + 1, "tp", other, block, block).start()
        wait_bytes(recv.at[phase + 1], buf.at[0])

    def line_sum(dst):
        total = dst[0].astype(F32)
        for z in range(1, n_z):
            total = total + dst[z].astype(F32)
        return total

    local[25].wait()
    lane = lax.broadcasted_iota(jnp.int32, (rows, 128), 1)
    rowi = lax.broadcasted_iota(jnp.int32, (rows, 128), 0)
    half = ropew // 2
    freq = jnp.zeros((rows, 128), F32)
    for i in range(half):
        freq = jnp.where(lane % half == i, F32(ROPE_BASE ** (-i / half)), freq)
    pos = jnp.zeros((rows, 128), jnp.int32)
    for s in range(rows):
        pos = jnp.where(rowi == s, lengths[s], pos)
    angle = pos.astype(F32) * freq
    cosv = jnp.cos(angle)
    sinv = jnp.sin(angle)

    def rotated(v, c, s):
        ln = lax.broadcasted_iota(jnp.int32, v.shape, 1)
        other = jnp.where(
            ln % ropew < half, -pltpu.roll(v, 128 - half, 1), pltpu.roll(v, half, 1)
        )
        return v * c + other * s

    pl.semaphore_wait(barrier, (n_tp - 1) + (n_ep - 1))
    local[0].wait()
    for d in near(n_z):
        to = 2 * lax.rem(place + d, n_z) + 1 - core
        hop(0, "tp", to, xo, xa.at[place]).start()
    shared = ((10, w1, (2, 3, 4)), (11, wku, (6,)), (12, wvu, (10,)), (13, wao, (11,)))

    def share(parts):
        for phase, held, waits in parts:
            for i in waits:
                local[i].wait()
            hop(phase, "tp", other, held.at[core], held.at[core]).start()

    share(shared[:2])

    local[1].wait()
    local[5].wait()
    tok = xo[...].astype(F32)
    own_normed = normed_rows(tok, again[...]).astype(BF16)
    krs[...] = jnp.zeros_like(krs)
    krs[:, 0:ropew] = nt(own_normed, wkr[...])
    new_rope = rotated(krs[...], cosv, sinv).astype(BF16).astype(F32)
    nrope_o[...] = new_rope[:, 0:ropew].astype(BF16)
    local[7].wait()

    await_line(0, xa)
    for phase, held, _ in shared[:2]:
        wait_bytes(recv.at[phase], held.at[0])
    half_rows = rows * n_z
    part = big.at[pl.ds(0, half_rows)]
    for z in range(n_z):
        big[pl.ds(rows * z, rows), :] = xa[z].astype(F32)
    normed = normed_rows(part[...], again[...]).astype(BF16)
    y = nt(normed, w1[...].reshape(-1, width))
    for k in range(2):
        yk = y[:, 128 * k : 128 * k + 128]
        ql = nn(yk[:, 0:nope].astype(BF16), wku[k])
        put(pl.ds(0, half_rows), jnp.concatenate([ql, yk], axis=1))
        for z in range(n_z):
            bs[z, :, wide * k : wide * (k + 1)] = get(pl.ds(rows * z, rows), wide).astype(BF16)
    to_line(1, bs, br)
    share(shared[2:])
    local[8].wait()
    local[9].wait()
    await_line(1, br)
    for t in range(n_tp):
        put(pl.ds(rows * t, rows), br[t // 2, :, wide * (t % 2) : wide * (t % 2 + 1)].astype(F32))

    parts = []
    ln4 = lax.broadcasted_iota(jnp.int32, (rows, 128), 1)
    per = 128 // latw
    for k in range(latent // 128):
        acc = jnp.zeros((rows, 128), F32)
        for j in range(per):
            t = k * per + j
            at = wide * (t % 2) + latent
            piece = br[t // 2, :, at : at + 128].astype(F32)
            shift = (j * latw - (nope + ropew)) % 128
            if shift:
                piece = pltpu.roll(piece, shift, 1)
            acc = jnp.where(ln4 // latw == j, piece, acc)
        parts.append(acc)
    latent_raw = jnp.concatenate(parts, axis=1)
    nl16 = normed_rows(latent_raw, lgain[...]).astype(BF16)
    nlat_o[...] = nl16
    new_latent = nl16.astype(F32)
    lane_r = lax.broadcasted_iota(jnp.int32, (rows, 128), 1)
    nr_al = jnp.where(
        (lane_r >= nope) & (lane_r < nope + ropew), pltpu.roll(new_rope, nope, 1), 0.0
    )

    n_heads = n_tp
    nlr = [new_latent[s : s + 1] for s in range(rows)]
    qrots, owns = [], []
    for s in range(rows):
        q = get(pl.ds(s, n_heads, stride=rows), latent)
        qr = rf[latent // 128, pl.ds(s, n_heads, stride=rows), :]
        sco[s] = nt(q.astype(BF16), cache[s])
        qrot = rotated(qr, cosv[s : s + 1], sinv[s : s + 1]).astype(BF16).astype(F32)
        owns.append(
            (
                jnp.sum(q * nlr[s], axis=-1, keepdims=True)
                + jnp.sum(qrot * nr_al[s : s + 1], axis=-1, keepdims=True)
            )
            * scale
        )
        shift = (ropew * s - nope) % 128
        lnq = lax.broadcasted_iota(jnp.int32, qrot.shape, 1)
        qrots.append(
            jnp.where(lnq // ropew == s, pltpu.roll(qrot, shift, 1) if shift else qrot, 0.0)
        )
    qrbd = jnp.concatenate(qrots, axis=0).astype(BF16)
    srope = nn(qrbd, rope[...])
    own_w = []
    for s in range(rows):
        sc = (sco[s] + srope[n_heads * s : n_heads * (s + 1)]) * scale
        col = lax.broadcasted_iota(jnp.int32, (n_heads, length), 1)
        sc = jnp.where(col < lengths[s], sc, -jnp.inf)
        own = owns[s]
        peak = jnp.maximum(jnp.max(sc, axis=-1, keepdims=True), own)
        pe = jnp.exp(sc - peak)
        oe = jnp.exp(own - peak)
        inv = 1.0 / (jnp.sum(pe, axis=-1, keepdims=True) + oe)
        prob[s] = (pe * inv).astype(BF16)
        own_w.append((oe * inv).astype(BF16).astype(F32))
    for s in range(rows):
        out = nn(prob[s], cache[s]) + own_w[s] * nlr[s]
        put(pl.ds(n_heads * s, n_heads), out)
    for t in range(n_tp):
        at = latent * (t % 2)
        cs[t // 2, :, at : at + latent] = get(pl.ds(t, rows, stride=n_heads), latent).astype(BF16)
    to_line(2, cs, cr)
    for i in range(12, 16):
        local[i].wait()

    cap = fs.shape[1]
    slots = n_ep * cap
    sl = lax.broadcasted_iota(jnp.int32, (slots, group), 0)
    want = (sl // cap) * n_tp + other
    hit = jnp.zeros((slots, group), F32)
    wgt = jnp.zeros((slots, group), F32)
    for k in range(ids_h.shape[0]):
        m = ids[k : k + 1, :] == want
        hit = jnp.where(m, 1.0, hit)
        wgt = jnp.where(m, rw[k : k + 1, :], wgt)
    before = (
        lax.broadcasted_iota(jnp.int32, (group, group), 0)
        < lax.broadcasted_iota(jnp.int32, (group, group), 1)
    )
    rank = nn(hit.astype(BF16), jnp.where(before, 1.0, 0.0).astype(BF16))
    taken = (hit > 0.5) & (jnp.abs(rank - (sl % cap).astype(F32)) < 0.5)
    disp = jnp.where(taken, 1.0, 0.0).astype(BF16)
    comb = jnp.where(taken, wgt, 0.0)
    comb_hi = comb.astype(BF16)
    comb_lo = (comb - comb_hi.astype(F32)).astype(BF16)

    await_line(2, cr)
    for phase, held, _ in shared[2:]:
        wait_bytes(recv.at[phase], held.at[0])
    total = None
    for k in range(2):
        for z in range(n_z):
            put(pl.ds(rows * z, rows), cr[z, :, latent * k : latent * (k + 1)].astype(F32))
        hv = nt(get(pl.ds(0, half_rows), latent).astype(BF16), wvu[k]).astype(BF16)
        term = nn(hv, wao[k])
        total = term if total is None else total + term
    part[...] = total
    for z in range(n_z):
        ds_[z] = big[pl.ds(rows * z, rows), :].astype(BF16)
    to_line(3, ds_, dr)
    for i in range(16, 25):
        local[i].wait()
    await_line(3, dr)
    after = tok + line_sum(dr)
    ee[core, place] = normed_rows(after, fgain[...]).astype(BF16)
    gather(4, 0, ee)
    gather_rest(4, 0, ee)
    for t in range(n_tp):
        big[pl.ds(rows * t, rows), :] = ee[t % 2, t // 2].astype(F32)
    ffn = big[...].astype(BF16)
    out = nn(disp, ffn)
    small[...] = out
    for g in range(n_ep):
        fs[g] = small[pl.ds(cap * g, cap), :].astype(BF16)
    to_all_ep(6, fs, fr)
    gate = bg[...].astype(F32)
    dots = big[:, 0:128] * gate[0:1]
    for k in range(1, width // 128):
        dots = dots + big[:, 128 * k : 128 * k + 128] * gate[k : k + 1]
    mix = jax.nn.sigmoid(jnp.sum(dots, axis=-1, keepdims=True))
    h = nt(ffn, w2[...])
    a, b = sg_h.shape[0], dg_h.shape[0]
    sact = (silu(h[:, 0:a]) * h[:, a : 2 * a]).astype(BF16)
    dact = (silu(h[:, 2 * a : 2 * a + b]) * h[:, 2 * a + b : 2 * a + 2 * b]).astype(BF16)
    wait_bytes(recv.at[6], fr)
    for g in range(n_ep):
        small[pl.ds(cap * g, cap), :] = fr[g].astype(F32)
    arrived = small[...].astype(BF16)
    act = (silu(nn(arrived, eg[...])) * nn(arrived, eu[...])).astype(BF16)
    small[...] = nn(act, ed[...])
    for g in range(n_ep):
        gs[g] = small[pl.ds(cap * g, cap), :].astype(BF16)
    to_all_ep(7, gs, gr)
    big[...] = nn(sact, sd[...]) + mix * nn(dact, dd[...])
    wait_bytes(recv.at[7], gr)
    for g in range(n_ep):
        small[pl.ds(cap * g, cap), :] = gr[g].astype(F32)
    back = small[...].astype(BF16)
    big[...] += tn(comb_hi, back) + tn(comb_lo, back)
    def two(z):
        both = big[pl.ds(pl.multiple_of(2 * rows * z, 2 * rows), 2 * rows), :]
        low, high = both[0:rows], both[rows : 2 * rows]
        return jnp.where(core == 0, low, high), jnp.where(core == 0, high, low)

    order = [(d, lax.rem(place + d, n_z)) for d in near(n_z)]
    for d, z in order:
        hs[z] = two(z)[1].astype(BF16)
        hop(8, "tp", other, hs.at[z], hp.at[z], each.at[1, d]).start()
    for d, z in order:
        wait_bytes(each.at[1, d], hp.at[z])
        hm[z] = (two(z)[0] + hp[z].astype(F32)).astype(BF16)
        if d:
            hop(9, "tp", 2 * z + core, hm.at[z], hr.at[place]).start()
        else:
            hr[place] = hm[z]
    wait_bytes(send.at[4], ee.at[0, pl.ds(0, n_z - 1)])
    wait_bytes(send.at[5], ee.at[0])
    for phase, buf in ((0, xa), (1, bs), (2, cs), (3, ds_)):
        wait_bytes(send.at[phase], buf)
    for phase, buf in ((6, fs), (7, gs)):
        wait_bytes(send.at[phase], buf)
    wait_bytes(send.at[8], hp)
    for phase, held, _ in shared:
        wait_bytes(send.at[phase], held.at[0])
    wait_bytes(recv.at[9], hr.at[pl.ds(0, n_z - 1)])
    total = line_sum(hr)
    mixed_o[...] = (after + total).astype(BF16)
    wait_bytes(send.at[9], hm.at[pl.ds(0, n_z - 1)])


def local(
    tokens,
    lengths,
    cache_latent,
    cache_rope_key,
    route_ids,
    route_weights,
    attn_gain,
    w_query_nope,
    w_query_rope,
    w_latent_down,
    w_key_rope,
    latent_gain,
    w_key_up,
    w_value_up,
    w_attn_out,
    ffn_gain,
    expert_gate,
    expert_up,
    expert_down,
    shared_gate,
    shared_up,
    shared_down,
    dense_gate,
    dense_up,
    dense_down,
    branch_gate,
):
    n_tp = lax.axis_size("tp")
    n_ep = lax.axis_size("ep")
    rows, width = tokens.shape
    group = rows * n_tp
    wqn = w_query_nope.reshape(width, -1).T
    wqr = w_query_rope.reshape(width, -1).T
    wld = w_latent_down.T
    wkr = w_key_rope.T
    wku = w_key_up.reshape(w_key_up.shape[0], -1).T
    wvu = w_value_up.reshape(w_value_up.shape[0], -1).T
    wao = w_attn_out.reshape(-1, width)
    sg, su, dg, du = shared_gate.T, shared_up.T, dense_gate.T, dense_up.T
    rope = jnp.swapaxes(cache_rope_key, 1, 2).reshape(-1, cache_rope_key.shape[1])
    latent = wku.shape[1]
    ropew = wqr.shape[0]
    cap = max(2, -(-2 * rows * route_ids.shape[1] // n_ep))
    args = [
        lengths,
        tokens,
        cache_latent,
        rope,
        route_ids.T,
        route_weights.T,
        attn_gain.reshape(1, -1),
        wqn,
        wqr,
        wld,
        wkr,
        latent_gain.reshape(1, -1),
        wku,
        wvu,
        wao,
        ffn_gain.reshape(1, -1),
        expert_gate[0],
        expert_up[0],
        expert_down[0],
        sg,
        su,
        shared_down,
        dg,
        du,
        dense_down,
        branch_gate.reshape(-1, 128),
    ]
    hbm_spec = pl.BlockSpec(memory_space=pltpu.HBM)
    vm = lambda a: pltpu.VMEM(a.shape, a.dtype)
    n1 = wqn.shape[0] + ropew + wld.shape[0]
    n2 = 2 * (sg.shape[0] + dg.shape[0])
    wide = latent + 128
    scratch = [
        pltpu.SMEM(lengths.shape, jnp.int32),
        vm(cache_latent),
        vm(rope),
        vm(args[4]),
        vm(args[5]),
        vm(args[6]),
        pltpu.VMEM((2, n1, width), BF16),
        vm(wkr),
        vm(args[11]),
        pltpu.VMEM((2, *wku.shape), BF16),
        pltpu.VMEM((2, *wvu.shape), BF16),
        pltpu.VMEM((2, *wao.shape), BF16),
        vm(args[15]),
        vm(args[16]),
        vm(args[17]),
        vm(args[18]),
        pltpu.VMEM((n2, width), BF16),
        vm(shared_down),
        vm(dense_down),
        vm(args[25]),
        pltpu.VMEM((rows, width), BF16),
        pltpu.VMEM((n_tp // 2, rows, width), BF16),
        pltpu.VMEM((n_tp // 2, rows, 2 * wide), BF16),
        pltpu.VMEM((n_tp // 2, rows, 2 * wide), BF16),
        pltpu.VMEM((n_tp // 2, rows, 2 * latent), BF16),
        pltpu.VMEM((n_tp // 2, rows, 2 * latent), BF16),
        pltpu.VMEM((n_tp // 2, rows, width), BF16),
        pltpu.VMEM((n_tp // 2, rows, width), BF16),
        pltpu.VMEM((2, n_tp // 2, rows, width), BF16),
        pltpu.VMEM((n_ep, cap, width), BF16),
        pltpu.VMEM((n_ep, cap, width), BF16),
        pltpu.VMEM((n_ep, cap, width), BF16),
        pltpu.VMEM((n_ep, cap, width), BF16),
        pltpu.VMEM((n_tp // 2, rows, width), BF16),
        pltpu.VMEM((n_tp // 2, rows, width), BF16),
        pltpu.VMEM((n_tp // 2, rows, width), BF16),
        pltpu.VMEM((n_tp // 2, rows, width), BF16),
        pltpu.VMEM((rows, n_tp, cache_latent.shape[1]), F32),
        pltpu.VMEM((rows, n_tp, cache_latent.shape[1]), BF16),
        pltpu.VMEM((group, width), F32),
        pltpu.VMEM((n_ep * cap, width), F32),
        pltpu.VMEM((wide // 128, group, 128), F32),
        pltpu.VMEM((rows, 128), F32),
        pltpu.SemaphoreType.DMA((26,)),
        pltpu.SemaphoreType.DMA((14,)),
        pltpu.SemaphoreType.DMA((14,)),
        pltpu.SemaphoreType.DMA((2, n_tp // 2)),
    ]
    found = pl.pallas_call(
        functools.partial(layer_kernel, n_tp, n_ep),
        out_shape=(
            jax.ShapeDtypeStruct((rows, width), BF16),
            jax.ShapeDtypeStruct((rows, latent), BF16),
            jax.ShapeDtypeStruct((rows, ropew), BF16),
        ),
        in_specs=[hbm_spec] * 26,
        out_specs=(pl.BlockSpec(memory_space=pltpu.VMEM),) * 3,
        scratch_shapes=scratch,
        compiler_params=pltpu.CompilerParams(
            collective_id=0, has_side_effects=True, vmem_limit_bytes=40 * 1024 * 1024
        ),
        name="layer",
    )(*[pltpu.with_memory_space_constraint(a, pltpu.HBM) for a in args])
    vmem = pl.BlockSpec(memory_space=pltpu.VMEM)
    return pl.pallas_call(
        finish_kernel,
        out_shape=tuple(jax.ShapeDtypeStruct(a.shape, a.dtype) for a in found),
        in_specs=[vmem] * 3,
        out_specs=(vmem,) * 3,
        compiler_params=pltpu.CompilerParams(vmem_limit_bytes=8 * 1024 * 1024),
        name="finish",
    )(*found)


def solution(mesh):
    in_specs = (
        P(("ep", "tp"), None),
        P(("ep", "tp")),
        P(("ep", "tp"), None, None),
        P(("ep", "tp"), None, None),
        P("ep", None),
        P("ep", None),
        P(),
        P(None, "tp", None),
        P(None, "tp", None),
        P(None, "tp"),
        P(),
        P(),
        P(None, "tp", None),
        P(None, "tp", None),
        P("tp", None, None),
        P(),
        P(("ep", "tp"), None, None),
        P(("ep", "tp"), None, None),
        P(("ep", "tp"), None, None),
        P(None, "tp"),
        P(None, "tp"),
        P("tp", None),
        P(None, "tp"),
        P(None, "tp"),
        P("tp", None),
        P(),
    )
    out_specs = (P(("ep", "tp"), None), P(("ep", "tp"), None), P(("ep", "tp"), None))
    return jax.shard_map(local, mesh=mesh, in_specs=in_specs, out_specs=out_specs, check_vma=False)
```
